32 devices in a mesh: sp: 8 (over z, y), tp: 4 (over x, core).
Axes of the slice: x: 2, y: 2, z: 4, core: 2. Of those that a mesh axis runs over, the one named last changes fastest.
Arguments:
- hidden_states: bfloat16 [2048, 4096], P('sp', 'tp'), may hold values from -6 to 6
- norm_gain: float32 [4096], replicated, may hold values from 0.1 to 1.9
- query_weight: bfloat16 [4096, 2048], P('sp', 'tp'), may hold values from -0.09375 to 0.09375
- key_weight: bfloat16 [4096, 2048], P('sp', 'tp'), may hold values from -0.09375 to 0.09375
- value_weight: bfloat16 [4096, 2048], P('sp', 'tp'), may hold values from -0.09375 to 0.09375
- output_gate_weight: bfloat16 [4096, 2048], P('sp', 'tp'), may hold values from -0.09375 to 0.09375
- unit_input_weight: bfloat16 [4096, 2048], P('sp', 'tp'), may hold values from -0.09375 to 0.09375
- unit_gate_weight: bfloat16 [4096, 2048], P('sp', 'tp'), may hold values from -0.09375 to 0.09375
- decay_forward: float32 [16], P('tp'), may hold values from 0 to 16
- decay_backward: float32 [16], P('tp'), may hold values from 0 to 16
- group_gain: float32 [2048], P('tp'), may hold values from 0.1 to 1.9
- group_bias: float32 [2048], P('tp'), may hold values from -3 to 3
- depth_kernel: float32 [31, 2048], P(None, 'tp'), may hold values from -7 to 7
- depth_bias: float32 [2048], P('tp'), may hold values from -3 to 3
- channel_gain: float32 [2048], P('tp'), may hold values from 0.1 to 1.9
- channel_bias: float32 [2048], P('tp'), may hold values from -3 to 3
- retention_out_weight: bfloat16 [2048, 4096], P('tp', 'sp'), may hold values from -0.09375 to 0.09375
- convolution_out_weight: bfloat16 [2048, 4096], P('tp', 'sp'), may hold values from -0.09375 to 0.09375
Outputs:
- mixed_out: bfloat16 [2048, 4096], P(('sp', 'tp'))
The draws below stay inside these ranges and needn't reach their ends.
All inputs are finite; a program needn't handle non-finite values.
Results may differ from the reference program's by a relative error of at most 0.018.
Values may be sent and summed in bfloat16 or wider, within the bound.
A program may use at most 128 MiB of HBM per device.

```python
import jax
import jax.numpy as jnp
from jax import lax

D = 4096
HEADS = 16
HEAD_DIM = 128
RET_WIDTH = 2048
CONV_WIDTH = 2048
KERNEL = 31
BLOCK = 128
TOKENS = 2048
N_TP = 4


def decay_logits(key, salt):
    key_pick, key_slow, key_fast = jax.random.split(jax.random.fold_in(key, salt), 3)
    keeps_state = jax.random.uniform(key_pick, (HEADS,), jnp.float32) < 0.5
    slow_rate = jnp.exp(jax.random.uniform(key_slow, (HEADS,), jnp.float32, jnp.log(0.2), jnp.log(2.0))) / TOKENS
    fast_rate = jnp.exp(jax.random.uniform(key_fast, (HEADS,), jnp.float32, jnp.log(1.0 / 100.0), jnp.log(1.0 / 30.0)))
    decay_rate = jnp.where(keeps_state, slow_rate, fast_rate)
    return -decay_rate - jnp.log(-jnp.expm1(-decay_rate))


def draw_decay_forward(key, part):
    return decay_logits(key, 11)


def draw_decay_backward(key, part):
    return decay_logits(key, 23)


def draw_depth_kernel(key, part):
    key_tap, key_spread = jax.random.split(jax.random.fold_in(key, 5))
    channel = jnp.arange(CONV_WIDTH, dtype=jnp.float32)
    rising = jnp.exp(jnp.log(3.0) * channel / CONV_WIDTH)
    spread = jnp.exp(jax.random.uniform(key_spread, (CONV_WIDTH,), jnp.float32, 0.0, jnp.log(4.0)))
    tap_values = jnp.clip(jax.random.normal(key_tap, (KERNEL, CONV_WIDTH), jnp.float32), -3.0, 3.0)
    return tap_values * (rising * spread)[None, :] / jnp.sqrt(jnp.float32(KERNEL))


def levels(own_key, shape, cuts, least, top_value):
    gain = 1.0
    for dim, blocks in cuts:
        heights = jax.random.uniform(jax.random.fold_in(jax.random.fold_in(own_key, 6), dim), (blocks,), jnp.float32, least / len(cuts), top_value / len(cuts))
        gain = gain * jnp.repeat(jnp.exp(heights), shape[dim] // blocks).reshape((-1,) + (1,) * (len(shape) - 1 - dim))
    return gain


def bell_draw(stream_key, extent, scale, most, shards=(), kind=jnp.bfloat16):
    entries = jax.random.normal(stream_key, extent, jnp.float32) * scale
    if len(shards) > 0:
        entries = levels(stream_key, extent, shards, -0.22, 0.18) * entries
    return jnp.clip(entries, min=-most, max=most).astype(kind)


def setup_inputs(seed: int = 0) -> dict:
    key_list = jax.random.split(jax.random.key(seed), 19)
    hidden_states = bell_draw(key_list[0], (TOKENS, D), 1.0, 6.0, ((0, 8), (1, 4)))
    norm_gain = jnp.clip(1.0 + 0.18 * jax.random.normal(key_list[1], (D,), jnp.float32), 0.1, 1.9)
    query_weight = bell_draw(key_list[2], (D, RET_WIDTH), D ** -0.5, 0.09375, ((0, 8), (1, 4)))
    key_weight = bell_draw(key_list[3], (D, RET_WIDTH), D ** -0.5, 0.09375, ((0, 8), (1, 4)))
    value_weight = bell_draw(key_list[4], (D, RET_WIDTH), D ** -0.5, 0.09375, ((0, 8), (1, 4)))
    output_gate_weight = bell_draw(key_list[5], (D, RET_WIDTH), D ** -0.5, 0.09375, ((0, 8), (1, 4)))
    unit_input_weight = bell_draw(key_list[6], (D, CONV_WIDTH), D ** -0.5, 0.09375, ((0, 8), (1, 4)))
    unit_gate_weight = bell_draw(key_list[7], (D, CONV_WIDTH), D ** -0.5, 0.09375, ((0, 8), (1, 4)))
    decay_forward = draw_decay_forward(jax.random.fold_in(key_list[18], 71), 0)
    decay_backward = draw_decay_backward(jax.random.fold_in(key_list[18], 71), 0)
    group_gain = jnp.clip(1.0 + 0.18 * jax.random.normal(key_list[10], (RET_WIDTH,), jnp.float32), 0.1, 1.9)
    group_bias = bell_draw(key_list[11], (RET_WIDTH,), 0.5, 3.0, ((0, 4),), jnp.float32)
    depth_kernel = draw_depth_kernel(jax.random.fold_in(key_list[18], 71), 0)
    depth_bias = bell_draw(key_list[13], (CONV_WIDTH,), 0.5, 3.0, ((0, 4),), jnp.float32)
    channel_gain = jnp.clip(1.0 + 0.18 * jax.random.normal(key_list[14], (CONV_WIDTH,), jnp.float32), 0.1, 1.9)
    channel_bias = bell_draw(key_list[15], (CONV_WIDTH,), 0.5, 3.0, ((0, 4),), jnp.float32)
    retention_out_weight = bell_draw(key_list[16], (RET_WIDTH, D), (RET_WIDTH + CONV_WIDTH) ** -0.5, 0.09375, ((0, 4), (1, 8)))
    convolution_out_weight = bell_draw(key_list[17], (CONV_WIDTH, D), (RET_WIDTH + CONV_WIDTH) ** -0.5, 0.09375, ((0, 4), (1, 8)))
    return dict(hidden_states=hidden_states, norm_gain=norm_gain, query_weight=query_weight, key_weight=key_weight, value_weight=value_weight, output_gate_weight=output_gate_weight, unit_input_weight=unit_input_weight, unit_gate_weight=unit_gate_weight, decay_forward=decay_forward, decay_backward=decay_backward, group_gain=group_gain, group_bias=group_bias, depth_kernel=depth_kernel, depth_bias=depth_bias, channel_gain=channel_gain, channel_bias=channel_bias, retention_out_weight=retention_out_weight, convolution_out_weight=convolution_out_weight)


EPS = 1e-06
THETA = 10000.0

def rotate(rows, positions):
    half_dim = rows.shape[-1] // 2
    inverse = THETA ** (-jnp.arange(half_dim, dtype=jnp.float32) / half_dim)
    angles = positions.astype(jnp.float32)[:, None] * inverse[None, :]
    cosine = jnp.cos(angles)[:, None, :]
    sine = jnp.sin(angles)[:, None, :]
    widened = rows.astype(jnp.float32)
    first_half = widened[..., :half_dim]
    second_half = widened[..., half_dim:]
    turned = jnp.concatenate([first_half * cosine - second_half * sine, second_half * cosine + first_half * sine], axis=-1)
    return turned.astype(jnp.bfloat16)

def to_blocks(rows):
    return rows.reshape(rows.shape[0] // BLOCK, BLOCK, rows.shape[1], rows.shape[2]).transpose(2, 0, 1, 3)

def from_blocks(blocks):
    return blocks.transpose(1, 2, 0, 3).reshape(blocks.shape[1] * blocks.shape[2], blocks.shape[0], blocks.shape[3])

def blockwise(queries, key_rows, values, log_decay, include_diag):
    block_len = queries.shape[2]
    position = jnp.arange(block_len, dtype=jnp.float32)
    distance = position[:, None] - position[None, :]
    allowed = distance >= 0 if include_diag else distance > 0
    inside = jnp.where(allowed[None], jnp.exp(log_decay[:, None, None] * jnp.maximum(distance, 0.0)[None]), 0.0)
    query_wide = queries.astype(jnp.float32)
    key_wide = key_rows.astype(jnp.float32)
    value_wide = values.astype(jnp.float32)
    scores = jnp.einsum('hnqd,hnkd->hnqk', query_wide, key_wide, precision=lax.Precision.HIGHEST) * inside[:, None]
    inner_part = jnp.einsum('hnqk,hnkd->hnqd', scores, value_wide, precision=lax.Precision.HIGHEST)
    toward_end = jnp.exp(log_decay[:, None] * (block_len - 1.0 - position)[None])
    block_states = jnp.einsum('hnkd,hnke->hnde', key_wide * toward_end[:, None, :, None], value_wide, precision=lax.Precision.HIGHEST)
    block_decay = jnp.exp(log_decay * block_len)[:, None, None]

    def advance(state_now, block_state):
        return (block_decay * state_now + block_state, state_now)
    initial = jnp.zeros((block_states.shape[0], block_states.shape[2], block_states.shape[3]), jnp.float32)
    final_state, earlier = lax.scan(advance, initial, jnp.moveaxis(block_states, 1, 0))
    earlier = jnp.moveaxis(earlier, 0, 1)
    from_start = jnp.exp(log_decay[:, None] * (position + 1.0)[None])
    cross_part = jnp.einsum('hnqd,hnde->hnqe', query_wide * from_start[:, None, :, None], earlier, precision=lax.Precision.HIGHEST)
    return (inner_part + cross_part, final_state)

def group_norm(retained, group_gain, group_bias, gate_rows):
    row_mean = lax.optimization_barrier(jnp.mean(retained, axis=-1, keepdims=True))
    centered = retained - row_mean
    variance = lax.optimization_barrier(jnp.mean(centered * centered, axis=-1, keepdims=True))
    scaled = (centered * lax.rsqrt(variance + EPS)).reshape(retained.shape[0], -1)
    scaled = scaled * group_gain[None, :] + group_bias[None, :]
    return (jax.nn.silu(gate_rows.astype(jnp.float32)) * scaled).astype(jnp.bfloat16)

def reference(hidden_states, norm_gain, query_weight, key_weight, value_weight, output_gate_weight, unit_input_weight, unit_gate_weight, decay_forward, decay_backward, group_gain, group_bias, depth_kernel, depth_bias, channel_gain, channel_bias, retention_out_weight, convolution_out_weight):
    widened = hidden_states.astype(jnp.float32)
    normed = (widened * lax.rsqrt(lax.optimization_barrier(jnp.mean(widened * widened, axis=-1, keepdims=True)) + EPS) * norm_gain[None, :]).astype(jnp.bfloat16)

    def project(weight):
        return jnp.dot(normed, weight, preferred_element_type=jnp.float32).astype(jnp.bfloat16)
    proj_q = project(query_weight)
    proj_k = project(key_weight)
    proj_v = project(value_weight)
    proj_g = project(output_gate_weight)
    proj_a = project(unit_input_weight)
    proj_b = project(unit_gate_weight)
    positions = jnp.arange(TOKENS, dtype=jnp.int32)
    queries = rotate(proj_q.reshape(TOKENS, HEADS, HEAD_DIM), positions)
    key_rows = rotate(proj_k.reshape(TOKENS, HEADS, HEAD_DIM), positions)
    values = proj_v.reshape(TOKENS, HEADS, HEAD_DIM)
    log_forward = jax.nn.log_sigmoid(decay_forward)
    log_backward = jax.nn.log_sigmoid(decay_backward)
    ahead, unused_ahead = blockwise(to_blocks(queries), to_blocks(key_rows), to_blocks(values), log_forward, True)
    behind, unused_behind = blockwise(to_blocks(queries[::-1]), to_blocks(key_rows[::-1]), to_blocks(values[::-1]), log_backward, False)
    retained = from_blocks(ahead) + from_blocks(behind)[::-1]
    retention_rows = group_norm(retained, group_gain, group_bias, proj_g)
    unit = (proj_a.astype(jnp.float32) * jax.nn.sigmoid(proj_b.astype(jnp.float32))).astype(jnp.bfloat16)
    half_kernel = (KERNEL - 1) // 2
    padded = jnp.pad(unit, ((half_kernel, half_kernel), (0, 0)))
    filtered = jnp.broadcast_to(depth_bias[None, :], (TOKENS, CONV_WIDTH))
    for offset in range(KERNEL):
        filtered = filtered + depth_kernel[offset][None, :] * padded[offset:offset + TOKENS].astype(jnp.float32)
    row_mean = lax.optimization_barrier(jnp.sum(filtered, axis=1, keepdims=True)) / CONV_WIDTH
    variance = lax.optimization_barrier(jnp.sum(filtered * filtered, axis=1, keepdims=True)) / CONV_WIDTH - row_mean * row_mean
    leveled = (filtered - row_mean) * lax.rsqrt(variance + EPS) * channel_gain[None, :] + channel_bias[None, :]
    convolution_rows = jax.nn.silu(leveled).astype(jnp.bfloat16)
    ret_group = RET_WIDTH // N_TP
    conv_group = CONV_WIDTH // N_TP
    mixed = jnp.zeros((TOKENS, D), jnp.float32)
    for group in range(N_TP):
        partial_value = jnp.dot(retention_rows[:, group * ret_group:(group + 1) * ret_group], retention_out_weight[group * ret_group:(group + 1) * ret_group], preferred_element_type=jnp.float32)
        partial_value = partial_value + jnp.dot(convolution_rows[:, group * conv_group:(group + 1) * conv_group], convolution_out_weight[group * conv_group:(group + 1) * conv_group], preferred_element_type=jnp.float32)
        rounded = lax.optimization_barrier(partial_value.astype(jnp.bfloat16))
        mixed = mixed + rounded.astype(jnp.float32)
    return mixed.astype(jnp.bfloat16)
```

```python
import functools

import jax
import jax.numpy as jnp
import numpy as np
from jax import lax
from jax.experimental import pallas as pl
from jax.experimental.pallas import tpu as pltpu
from jax.sharding import PartitionSpec as P

HEAD_DIM = 128
CONV_WIDTH = 2048
KERNEL = 31

EPS = 1e-06
THETA = 10000.0
SIDES = 2
CORES = 2
BLOCK = 128
F32, BF16 = jnp.float32, jnp.bfloat16


class Copies:
    def __init__(self, sems):
        self.sems = sems
        self.used = 0
        self.pending = []

    def make(self, src, dst, arrived, device):
        copy = pltpu.make_async_remote_copy(
            src_ref=src,
            dst_ref=dst,
            send_sem=self.sems.at[self.used],
            recv_sem=arrived,
            device_id=device,
            device_id_type=pl.DeviceIdType.MESH,
        )
        self.used += 1
        return copy

    def send(self, src, dst, arrived, device, when=None):
        copy = self.make(src, dst, arrived, device)
        self.pending.append((copy, when))
        if when is None:
            copy.start()
        else:
            pl.when(when)(copy.start)

    def drain(self):
        for copy, when in self.pending:
            if when is None:
                copy.wait_send()
            else:
                pl.when(when)(copy.wait_send)


def fused_kernel(
    nz, half, n_tp, hid, gain, wq, wk, wv, wg, wa, wb, dec_f, dec_b, gg, gb, taps, dbias, cg, cb,
    wro, wco, table, out,
    xb, xg, ssq, wbuf, pj, ubuf, hs, hr, fbuf, st, sr, tb, ef, eb, ts, tr, kr, dcol, dmat, mix,
    wo, ps, r1, s2, r2, ob, os_,
    sends, lsem, rx_line, rx_y, rx_x, rx_c, rw_z, rw_y, r_wo, r_halo, r_stat, r_state, rm_c, rm_r,
    rs1, rs2, ro,
):
    sp, tp = lax.axis_index("sp"), lax.axis_index("tp")
    z, y, x, c = sp // SIDES, sp % SIDES, tp // CORES, tp % CORES
    blk, feats = hid.shape
    depth = wq.shape[0]
    rows = nz * blk
    lanes = HEAD_DIM
    fine = out.shape[0]
    chunks = nz
    cols = SIDES * wro.shape[1]
    cp = Copies(sends)

    def dev(x_, y_, z_, c_):
        return (z_ * SIDES + y_, x_ * CORES + c_)

    other_x, other_y, other_c = dev(1 - x, y, z, c), dev(x, 1 - y, z, c), dev(x, y, z, 1 - c)
    here = dev(x, y, z, c)
    me = z * n_tp + tp
    group = nz * n_tp

    def arrive(dst, sem):
        pltpu.make_async_remote_copy(
            src_ref=dst, dst_ref=dst, send_sem=sem, recv_sem=sem,
            device_id=here, device_id_type=pl.DeviceIdType.MESH,
        ).wait_recv()

    def aligned(value, step):
        return pl.multiple_of(value, step)

    pairs = ((wa, wb), (wk, wv), (wq, wg))
    own_slot = jnp.where(z // SIDES == y, tp * nz + (z % SIDES) * SIDES + y, n_tp * nz + z % SIDES)
    local = [pltpu.make_async_copy(hid, xb.at[own_slot], lsem.at[0])]
    my_cols = pl.ds(aligned(z * lanes, lanes), lanes)
    my_depth = pl.ds(aligned(sp * depth, depth), depth)
    for p, pair in enumerate(pairs):
        for j, weight in enumerate(pair):
            local.append(
                pltpu.make_async_copy(
                    weight.at[:, my_cols],
                    wbuf.at[p, my_depth, pl.ds(j * lanes, lanes)],
                    lsem.at[1 + 2 * p + j],
                )
            )
    side_cols = pl.ds(aligned(y * (cols // SIDES), cols // SIDES), cols // SIDES)
    for k in range(nz):
        for j, weight in enumerate((wro, wco)):
            local.append(
                pltpu.make_async_copy(
                    weight.at[pl.ds(k * lanes, lanes)],
                    wo.at[pl.ds((2 * k + j) * lanes, lanes), side_cols],
                    lsem.at[7 + 2 * k + j],
                )
            )
    local.append(
        pltpu.make_async_copy(
            table.at[pl.ds(aligned(y * rows, rows), rows)], tb, lsem.at[7 + 2 * nz]
        )
    )
    for copy in local:
        copy.start()

    barrier = pltpu.get_barrier_semaphore()
    for k in range(1, group):
        idx = (me + k) % group
        pl.semaphore_signal(
            barrier, inc=1, device_id=((idx // n_tp) * SIDES + y, idx % n_tp),
            device_id_type=pl.DeviceIdType.MESH,
        )
    for k in range(nz):
        pl.semaphore_signal(
            barrier, inc=1, device_id=(k * SIDES + 1 - y, tp),
            device_id_type=pl.DeviceIdType.MESH,
        )
    pl.semaphore_wait(barrier, group - 1 + nz)

    def is_mine(zz):
        return zz // SIDES == y

    def line_slot(zz):
        return jnp.where(
            is_mine(zz), tp * nz + (zz % SIDES) * SIDES + y, n_tp * nz + zz % SIDES
        )

    def both(a, b):
        return b if a is None else jnp.logical_and(a, b)

    def send_line(zz, step, when):
        slot = xb.at[line_slot(zz)]
        cp.send(slot, slot, rx_line.at[zz], dev(x, y, z + step, c), when)

    def share(b, when):
        slot = xb.at[tp * nz + b]
        cp.send(slot, slot, rx_x.at[b], other_x, when)
        cp.send(slot, slot, rx_c.at[b], other_c, when)

    def forward(zz, when=None):
        mine = is_mine(zz)
        cp.send(
            xb.at[n_tp * nz + zz % SIDES], xb.at[tp * nz + (zz % SIDES) * SIDES + y],
            rx_y.at[zz % SIDES], other_y, both(when, jnp.logical_not(mine)),
        )
        share((zz % SIDES) * SIDES + y, both(when, mine))

    def send_weights(p):
        for k in range(1, nz):
            zz = (z + k) % nz
            for j, weight in enumerate(pairs[p]):
                cp.send(
                    weight.at[:, pl.ds(aligned(zz * lanes, lanes), lanes)],
                    wbuf.at[p, my_depth, pl.ds(j * lanes, lanes)],
                    rw_z.at[p, z], dev(x, y, zz, c),
                )

    def weight_slice(p, zz, side):
        return wbuf.at[p, pl.ds(aligned((zz * SIDES + side) * depth, depth), depth)]

    def cross_weights(p):
        for k in range(1, nz):
            zz = (z + k) % nz
            piece = weight_slice(p, zz, y)
            arrive(piece, rw_z.at[p, zz])
            cp.send(piece, piece, rw_y.at[p, zz], other_y)

    def await_weights(p):
        for zz in range(nz):
            arrive(weight_slice(p, zz, 1 - y), rw_y.at[p, zz])

    local[0].wait()
    send_line(z, 1, z < nz - 1)
    send_line(z, -1, z > 0)
    forward(z)
    for p in range(3):
        local[1 + 2 * p].wait()
        local[2 + 2 * p].wait()
        piece = weight_slice(p, z, y)
        cp.send(piece, piece, rw_y.at[p, z], other_y)

    def y_arrivals(distance):
        for k in range(SIDES):
            zz = SIDES * y + k
            there = jnp.abs(z - zz) == distance
            b = k * SIDES + 1 - y
            pl.when(there)(lambda b=b, k=k: arrive(xb.at[tp * nz + b], rx_y.at[k]))
            share(b, there)

    for d in range(1, nz):
        low, high = z - d, z + d
        has_low, has_high = low >= 0, high < nz
        pl.when(has_low)(lambda low=low: arrive(xb.at[line_slot(low)], rx_line.at[low]))
        if d < nz - 1:
            send_line(low, 1, both(has_low, z < nz - 1))
        pl.when(has_high)(lambda high=high: arrive(xb.at[line_slot(high)], rx_line.at[high]))
        if d < nz - 1:
            send_line(high, -1, both(has_high, z > 0))
        forward(low, has_low)
        forward(high, has_high)
        y_arrivals(d - 1)
        if d == 1:
            send_weights(0)
        if d == 2:
            send_weights(1)
            send_weights(2)
    y_arrivals(nz - 1)

    def pick(ref):
        here_lane = lax.broadcasted_iota(jnp.int32, ref.shape, 1) == z
        v = jnp.sum(jnp.where(here_lane, ref[...], 0.0), axis=1, keepdims=True)
        e = jnp.exp(-jnp.abs(v))
        small = e * (1.0 - e * (0.5 - e * (1.0 / 3.0 - e * 0.25)))
        return jnp.minimum(v, 0.0) - jnp.where(e < 1e-2, small, jnp.log(1.0 + e))

    log_f, log_b = pick(dec_f), pick(dec_b)
    index = lax.broadcasted_iota(jnp.int32, (blk, lanes), 0).astype(F32)
    dcol[0] = jnp.exp(log_f * (blk - 1.0 - index))
    dcol[1] = jnp.exp(log_b * index)
    dcol[2] = jnp.exp(log_f * (index + 1.0))
    dcol[3] = jnp.exp(log_b * (blk - index))
    across = lax.broadcasted_iota(jnp.int32, (blk, blk), 0) - lax.broadcasted_iota(
        jnp.int32, (blk, blk), 1
    )
    away = across.astype(F32)
    dmat[...] = jnp.exp(jnp.where(across >= 0, log_f * away, -log_b * away))
    leap_f, leap_b = jnp.exp(log_f * float(blk)), jnp.exp(log_b * float(blk))

    def gather_squares(q, first):
        at = pl.ds(aligned(q * feats, feats), feats)

        def strip(i, carry):
            r = pl.ds(aligned(i * 16, 16), 16)
            v = xb[q * nz + i // (blk // 16), pl.ds(aligned((i % (blk // 16)) * 16, 16), 16)]
            v = v.astype(F32)
            xg[r, at] = (v * gain[:, at]).astype(BF16)
            w = v * v
            s = w[:, :lanes]
            for k in range(1, feats // lanes):
                s = s + w[:, k * lanes : (k + 1) * lanes]
            ssq[r] = s if first else ssq[r] + s
            return carry

        lax.fori_loop(0, rows // 16, strip, 0)

    cross_weights(0)
    gather_squares(tp, True)
    far_q = dev(1 - x, y, z, c)[1]
    for b in range(nz):
        slot = xb.at[far_q * nz + b]
        arrive(slot, rx_x.at[b])
        cp.send(slot, slot, rx_c.at[nz + b], other_c)
    gather_squares(far_q, False)
    for k, q in enumerate((dev(x, y, z, 1 - c)[1], dev(1 - x, y, z, 1 - c)[1])):
        for b in range(nz):
            arrive(xb.at[q * nz + b], rx_c.at[k * nz + b])
        gather_squares(q, False)

    width = n_tp * feats

    def finish(i, carry):
        r = pl.ds(aligned(i * 128, 128), 128)
        total = jnp.sum(ssq[r], axis=1, keepdims=True)
        ssq[r] = jnp.broadcast_to(lax.rsqrt(total / width + EPS), (128, lanes))
        return carry

    lax.fori_loop(0, rows // 128, finish, 0)

    def project(p):
        tall = 2 * blk

        def body(i, carry):
            r = pl.ds(aligned(i * tall, tall), tall)
            scale = ssq[r]
            acc = jnp.dot(xg[r], wbuf[p], preferred_element_type=F32)
            pj[p, r, pl.ds(0, lanes)] = (acc[:, :lanes] * scale).astype(BF16)
            pj[p, r, pl.ds(lanes, lanes)] = (acc[:, lanes:] * scale).astype(BF16)
            return carry

        lax.fori_loop(0, rows // tall, body, 0)

    await_weights(0)
    project(0)

    pad = 16
    ubuf[pl.ds(0, pad)] = jnp.zeros((pad, lanes), F32)
    ubuf[pl.ds(pad + rows, pad)] = jnp.zeros((pad, lanes), F32)

    def gate(i, carry):
        r = aligned(i * 128, 128)
        a = pj[0, pl.ds(r, 128), pl.ds(0, lanes)].astype(F32)
        b = pj[0, pl.ds(r, 128), pl.ds(lanes, lanes)].astype(F32)
        ubuf[pl.ds(aligned(r + pad, 16), 128)] = (a * jax.nn.sigmoid(b)).astype(BF16).astype(F32)
        return carry

    lax.fori_loop(0, rows // 128, gate, 0)
    edge = jnp.where(y == 0, rows, pad)
    hs[...] = ubuf[pl.ds(aligned(edge, 16), pad)].astype(BF16)
    cp.send(hs, hr, r_halo, other_y)
    wts = taps[:, my_cols]
    bias = dbias[:, my_cols]
    count = rows // 128
    reach = (KERNEL - 1) // 2

    def convolve(i, carry):
        block = jnp.where(y == 0, i, count - 1 - i)
        for part in range(2):
            r = aligned(block * 128 + part * 64, 64)
            acc = jnp.broadcast_to(bias, (64, lanes))
            for t in range(KERNEL):
                acc = acc + wts[t : t + 1] * ubuf[pl.ds(r + (pad - reach + t), 64)]
            fbuf[pl.ds(r, 64)] = acc
        turned = fbuf[pl.ds(aligned(block * 128, 128), 128)].T
        st[pl.ds(block, 1)] = jnp.sum(turned, axis=0, keepdims=True)
        st[pl.ds(count + block, 1)] = jnp.sum(turned * turned, axis=0, keepdims=True)
        return carry

    lax.fori_loop(0, count - 1, convolve, 0)
    arrive(hr, r_halo)
    got = hr[...].astype(F32)
    ubuf[pl.ds(0, pad)] = jnp.where(y == 1, got, 0.0)
    ubuf[pl.ds(pad + rows, pad)] = jnp.where(y == 0, got, 0.0)
    lax.fori_loop(count - 1, count, convolve, 0)
    for k in range(1, group):
        idx = (me + k) % group
        cp.send(
            st, sr.at[me], r_stat.at[me], ((idx // n_tp) * SIDES + y, idx % n_tp)
        )
    sr[me] = st[...]
    for k in range(1, group):
        idx = (me + k) % group
        arrive(sr.at[idx], r_stat.at[idx])
    sums = sr[0]
    for k in range(1, group):
        sums = sums + sr[k]
    st_mean = sums[:count] / CONV_WIDTH
    st_scale = lax.rsqrt(sums[count:] / CONV_WIDTH - st_mean * st_mean + EPS)
    conv_cols = pl.ds(aligned(z * 2 * lanes + lanes, lanes), lanes)
    ret_cols = pl.ds(aligned(z * 2 * lanes, lanes), lanes)
    gain_c, bias_c = cg[:, my_cols], cb[:, my_cols]
    for i in range(count):
        r = pl.ds(i * 128, 128)
        mean = jnp.broadcast_to(st_mean[i : i + 1], (128, lanes)).T
        scale = jnp.broadcast_to(st_scale[i : i + 1], (128, lanes)).T
        level = (fbuf[r] - mean) * scale * gain_c + bias_c
        mix[r, conv_cols] = (level * jax.nn.sigmoid(level)).astype(BF16)

    def mix_part(zz, r, conv):
        start = zz * 2 * lanes + (lanes if conv else 0)
        return mix.at[r, pl.ds(aligned(start, lanes), lanes)]

    def mix_send(zz, r, conv, sem, step, when):
        part = mix_part(zz, r, conv)
        cp.send(part, part, sem, dev(x, y, z + step, c), when)

    def mix_hop(d, r, conv, sems):
        low, high = z - d, z + d
        has_low, has_high = low >= 0, high < nz
        pl.when(has_low)(lambda: arrive(mix_part(low, r, conv), sems.at[low]))
        if d < nz - 1:
            mix_send(low, r, conv, sems.at[low], 1, both(has_low, z < nz - 1))
        pl.when(has_high)(lambda: arrive(mix_part(high, r, conv), sems.at[high]))
        if d < nz - 1:
            mix_send(high, r, conv, sems.at[high], -1, both(has_high, z > 0))

    every = pl.ds(0, rows)
    mix_send(z, every, True, rm_c.at[z], 1, z < nz - 1)
    mix_send(z, every, True, rm_c.at[z], -1, z > 0)

    cross_weights(1)
    await_weights(1)
    project(1)
    first_half = lax.broadcasted_iota(jnp.int32, (blk, lanes), 1) < lanes // 2

    def turn(v, r):
        t = tb[r]
        rolled = pltpu.roll(t, lanes // 2, 1)
        cosine = jnp.where(first_half, t, rolled)
        sine = jnp.where(first_half, -rolled, t)
        return (v * cosine + pltpu.roll(v, lanes // 2, 1) * sine).astype(BF16)

    local[-1].wait()

    def states(i, carry):
        r = pl.ds(aligned(i * blk, blk), blk)
        keys = turn(pj[1, r, pl.ds(0, lanes)].astype(F32), r)
        kr[r] = keys
        wide = keys.astype(F32)
        both_ways = jnp.concatenate(
            [(wide * dcol[0]).astype(BF16), (wide * dcol[1]).astype(BF16)], axis=1
        )
        state = lax.dot_general(
            both_ways, pj[1, r, pl.ds(lanes, lanes)], (((0,), (0,)), ((), ())),
            preferred_element_type=F32,
        )
        ef[i] = state[:lanes]
        eb[i] = state[lanes:]
        return carry

    lax.fori_loop(0, chunks, states, 0)
    run = ef[0]
    ef[0] = jnp.zeros_like(run)
    for i in range(1, chunks):
        own = ef[i]
        ef[i] = run
        run = run * leap_f + own
    back = eb[chunks - 1]
    eb[chunks - 1] = jnp.zeros_like(back)
    for i in range(chunks - 2, -1, -1):
        own = eb[i]
        eb[i] = back
        back = back * leap_b + own
    ts[...] = jnp.where(y == 0, run, back).astype(BF16)
    cp.send(ts, tr, r_state, other_y)

    cross_weights(2)
    for copy in local[7:-1]:
        copy.wait()
    piece = wo.at[:, side_cols]
    cp.send(piece, piece, r_wo, other_y)
    mix_hop(1, every, True, rm_c)
    arrive(tr, r_state)
    entering = tr[...].astype(F32)
    entering_f = jnp.where(y == 1, entering, 0.0)
    entering_b = jnp.where(y == 0, entering, 0.0)
    for i in range(chunks):
        ef[i] = ef[i] + entering_f
        entering_f = entering_f * leap_f
    for i in range(chunks - 1, -1, -1):
        eb[i] = eb[i] + entering_b
        entering_b = entering_b * leap_b
    await_weights(2)
    project(2)
    mix_hop(2, every, True, rm_c)
    gain_r, bias_r = gg[:, my_cols], gb[:, my_cols]

    def retain(i, carry):
        r = pl.ds(aligned(i * blk, blk), blk)
        queries = turn(pj[2, r, pl.ds(0, lanes)].astype(F32), r)
        keys, values = kr[r], pj[1, r, pl.ds(lanes, lanes)]
        scores = lax.dot_general(
            queries, keys, (((1,), (1,)), ((), ())), preferred_element_type=F32
        )
        scores = (scores * dmat[...]).astype(BF16)
        inner = jnp.dot(scores, values, preferred_element_type=F32)
        enter = jnp.concatenate([ef[i], eb[i]], axis=1).astype(BF16)
        carried = jnp.dot(queries, enter, preferred_element_type=F32)
        retained = inner + carried[:, :lanes] * dcol[2] + carried[:, lanes:] * dcol[3]
        mean = jnp.mean(retained, axis=-1, keepdims=True)
        centered = retained - mean
        spread = jnp.mean(centered * centered, axis=-1, keepdims=True)
        scaled = centered * lax.rsqrt(spread + EPS) * gain_r + bias_r
        g = pj[2, r, pl.ds(lanes, lanes)].astype(F32)
        mix[r, ret_cols] = (g * jax.nn.sigmoid(g) * scaled).astype(BF16)
        return carry

    spans = [pl.ds(i * blk, blk) for i in range(chunks)]
    for i in range(chunks):
        lax.fori_loop(i, i + 1, retain, 0)
        mix_send(z, spans[i], False, rm_r.at[i, z], 1, z < nz - 1)
        mix_send(z, spans[i], False, rm_r.at[i, z], -1, z > 0)
    mix_hop(3, every, True, rm_c)
    for d in range(1, nz - 1):
        for i in range(chunks):
            mix_hop(d, spans[i], False, rm_r.at[i])
    arrive(wo.at[:, pl.ds(aligned((1 - y) * (cols // SIDES), cols // SIDES), cols // SIDES)], r_wo)

    def multiply(i):
        mix_hop(nz - 1, spans[i], False, rm_r.at[i])
        acc = jnp.dot(mix[spans[i]], wo[...], preferred_element_type=F32)
        for t in range(n_tp):
            ps[i, t % CORES, t // CORES] = acc[t * fine : (t + 1) * fine].astype(BF16)
        cp.send(ps.at[i, 1 - c], r1.at[i], rs1.at[i], other_c)

    def add_cores(i):
        arrive(r1.at[i], rs1.at[i])
        s2[i] = (ps[i, c, 1 - x].astype(F32) + r1[i, 1 - x].astype(F32)).astype(BF16)
        cp.send(s2.at[i], r2.at[i], rs2.at[i], other_x)

    def add_far(i):
        arrive(r2.at[i], rs2.at[i])
        total = ps[i, c, x].astype(F32) + r1[i, x].astype(F32) + r2[i].astype(F32)
        os_[i] = total.astype(BF16)
        target = SIDES * nz // 2 * y + i
        away_ = target != sp
        cp.send(os_.at[i], ob.at[z], ro.at[z], (target, tp), away_)

        @pl.when(jnp.logical_not(away_))
        def _():
            ob[z] = os_[i]

    for i in range(chunks + 2):
        if i < chunks:
            multiply(i)
        if 0 <= i - 1 < chunks:
            add_cores(i - 1)
        if 0 <= i - 2 < chunks:
            add_far(i - 2)
    source_side = z // SIDES
    for zz in range(nz):
        @pl.when(jnp.logical_not(jnp.logical_and(zz == z, source_side == y)))
        def _():
            arrive(ob.at[zz], ro.at[zz])

        out[:, pl.ds(zz * cols, cols)] = ob[zz]
    cp.drain()


def fused(
    hidden_states, norm_gain, query_weight, key_weight, value_weight, output_gate_weight,
    unit_input_weight, unit_gate_weight, decay_forward, decay_backward, group_gain, group_bias,
    depth_kernel, depth_bias, channel_gain, channel_bias, retention_out_weight,
    convolution_out_weight,
):
    n_sp, n_tp = lax.axis_size("sp"), lax.axis_size("tp")
    nz = n_sp // SIDES
    blk, feats = hidden_states.shape
    depth = query_weight.shape[0]
    rows = nz * blk
    lanes = HEAD_DIM
    cols = SIDES * retention_out_weight.shape[1]
    fine = blk // n_tp
    half_dim = lanes // 2
    inverse = np.float32(THETA) ** (-np.arange(half_dim, dtype=np.float32) / np.float32(half_dim))
    angles = np.arange(SIDES * rows, dtype=np.float32)[:, None] * inverse.astype(np.float32)[None]
    table = np.concatenate([np.cos(angles.astype(np.float64)), np.sin(angles.astype(np.float64))], 1)
    table = jnp.asarray(table.astype(np.float32))
    count = rows // 128

    def row(v):
        return v.reshape(1, v.shape[0])

    any_, vmem = pl.BlockSpec(memory_space=pl.ANY), pl.BlockSpec(memory_space=pltpu.VMEM)
    dma = pltpu.SemaphoreType.DMA
    group = nz * n_tp
    return pl.pallas_call(
        functools.partial(fused_kernel, nz, SIDES, n_tp),
        out_shape=jax.ShapeDtypeStruct((fine, nz * cols), BF16),
        in_specs=[any_, vmem] + [any_] * 6 + [vmem] * 8 + [any_] * 3,
        out_specs=vmem,
        scratch_shapes=[
            pltpu.VMEM((n_tp * nz + SIDES, blk, feats), BF16),
            pltpu.VMEM((rows, n_tp * feats), BF16),
            pltpu.VMEM((rows, lanes), F32),
            pltpu.VMEM((3, n_sp * depth, 2 * lanes), BF16),
            pltpu.VMEM((3, rows, 2 * lanes), BF16),
            pltpu.VMEM((rows + 32, lanes), F32),
            pltpu.VMEM((16, lanes), BF16),
            pltpu.VMEM((16, lanes), BF16),
            pltpu.VMEM((rows, lanes), F32),
            pltpu.VMEM((2 * count, lanes), F32),
            pltpu.VMEM((group, 2 * count, lanes), F32),
            pltpu.VMEM((rows, lanes), F32),
            pltpu.VMEM((nz, lanes, lanes), F32),
            pltpu.VMEM((nz, lanes, lanes), F32),
            pltpu.VMEM((lanes, lanes), BF16),
            pltpu.VMEM((lanes, lanes), BF16),
            pltpu.VMEM((rows, lanes), BF16),
            pltpu.VMEM((4, blk, lanes), F32),
            pltpu.VMEM((blk, blk), F32),
            pltpu.VMEM((rows, nz * 2 * lanes), BF16),
            pltpu.VMEM((nz * 2 * lanes, cols), BF16),
            pltpu.VMEM((nz, CORES, n_tp // CORES, fine, cols), BF16),
            pltpu.VMEM((nz, n_tp // CORES, fine, cols), BF16),
            pltpu.VMEM((nz, fine, cols), BF16),
            pltpu.VMEM((nz, fine, cols), BF16),
            pltpu.VMEM((nz, fine, cols), BF16),
            pltpu.VMEM((nz, fine, cols), BF16),
            dma((200,)),
            dma((8 + 2 * nz,)),
            dma((nz,)), dma((SIDES,)), dma((nz,)), dma((2 * nz,)),
            dma((3, nz)), dma((3, nz)),
            dma, dma, dma((group,)), dma,
            dma((nz,)), dma((nz, nz)),
            dma((nz,)), dma((nz,)), dma((nz,)),
        ],
        compiler_params=pltpu.CompilerParams(
            collective_id=0, has_side_effects=True, vmem_limit_bytes=60 * 1024 * 1024
        ),
    )(
        hidden_states, row(norm_gain), query_weight, key_weight, value_weight, output_gate_weight,
        unit_input_weight, unit_gate_weight, row(decay_forward), row(decay_backward),
        row(group_gain), row(group_bias), depth_kernel, row(depth_bias), row(channel_gain),
        row(channel_bias), retention_out_weight, convolution_out_weight, table,
    )


def with_halo(cells, sides, width):
    for axis, dim in sides:
        count = lax.axis_size(axis)
        ends = count - 1
        head = lax.slice_in_dim(cells, 0, width, axis=dim)
        tail = lax.slice_in_dim(cells, cells.shape[dim] - width, cells.shape[dim], axis=dim)
        cells = jnp.concatenate(
            [
                lax.ppermute(tail, axis, [(i, (i + 1) % count) for i in range(ends)]),
                cells,
                lax.ppermute(head, axis, [((i + 1) % count, i) for i in range(ends)]),
            ],
            axis=dim,
        )
    return cells


def rotate_at(rows, positions):
    half_dim = rows.shape[-1] // 2
    inverse = THETA ** (-jnp.arange(half_dim, dtype=jnp.float32) / half_dim)
    angles = positions.astype(jnp.float32)[:, None] * inverse[None, :]
    cosine = jnp.cos(angles)[:, None, :]
    sine = jnp.sin(angles)[:, None, :]
    widened = rows.astype(jnp.float32)
    first_half = widened[..., :half_dim]
    second_half = widened[..., half_dim:]
    turned = jnp.concatenate(
        [first_half * cosine - second_half * sine, second_half * cosine + first_half * sine],
        axis=-1,
    )
    return turned.astype(jnp.bfloat16)


def to_blocks(rows):
    return rows.reshape(rows.shape[0] // BLOCK, BLOCK, rows.shape[1], rows.shape[2]).transpose(
        2, 0, 1, 3
    )


def from_blocks(blocks):
    return blocks.transpose(1, 2, 0, 3).reshape(
        blocks.shape[1] * blocks.shape[2], blocks.shape[0], blocks.shape[3]
    )


def blockwise(queries, key_rows, values, log_decay, include_diag):
    block_len = queries.shape[2]
    position = jnp.arange(block_len, dtype=jnp.float32)
    distance = position[:, None] - position[None, :]
    allowed = distance >= 0 if include_diag else distance > 0
    inside = jnp.where(
        allowed[None], jnp.exp(log_decay[:, None, None] * jnp.maximum(distance, 0.0)[None]), 0.0
    )
    query_wide = queries.astype(jnp.float32)
    key_wide = key_rows.astype(jnp.float32)
    value_wide = values.astype(jnp.float32)
    scores = (
        jnp.einsum("hnqd,hnkd->hnqk", query_wide, key_wide, precision=lax.Precision.HIGHEST)
        * inside[:, None]
    )
    inner_part = jnp.einsum("hnqk,hnkd->hnqd", scores, value_wide, precision=lax.Precision.HIGHEST)
    toward_end = jnp.exp(log_decay[:, None] * (block_len - 1.0 - position)[None])
    block_states = jnp.einsum(
        "hnkd,hnke->hnde",
        key_wide * toward_end[:, None, :, None],
        value_wide,
        precision=lax.Precision.HIGHEST,
    )
    block_decay = jnp.exp(log_decay * block_len)[:, None, None]

    def advance(state_now, block_state):
        return (block_decay * state_now + block_state, state_now)

    initial = jnp.zeros(
        (block_states.shape[0], block_states.shape[2], block_states.shape[3]), jnp.float32
    )
    final_state, earlier = lax.scan(advance, initial, jnp.moveaxis(block_states, 1, 0))
    earlier = jnp.moveaxis(earlier, 0, 1)
    from_start = jnp.exp(log_decay[:, None] * (position + 1.0)[None])
    cross_part = jnp.einsum(
        "hnqd,hnde->hnqe",
        query_wide * from_start[:, None, :, None],
        earlier,
        precision=lax.Precision.HIGHEST,
    )
    return (inner_part + cross_part, final_state)


def group_norm(retained, group_gain, group_bias, gate_rows):
    row_mean = jnp.mean(retained, axis=-1, keepdims=True)
    centered = retained - row_mean
    variance = jnp.mean(centered * centered, axis=-1, keepdims=True)
    scaled = (centered * lax.rsqrt(variance + EPS)).reshape(retained.shape[0], -1)
    scaled = scaled * group_gain[None, :] + group_bias[None, :]
    return (jax.nn.silu(gate_rows.astype(jnp.float32)) * scaled).astype(jnp.bfloat16)


def shards_general(
    hidden_states,
    norm_gain,
    query_weight,
    key_weight,
    value_weight,
    output_gate_weight,
    unit_input_weight,
    unit_gate_weight,
    decay_forward,
    decay_backward,
    group_gain,
    group_bias,
    depth_kernel,
    depth_bias,
    channel_gain,
    channel_bias,
    retention_out_weight,
    convolution_out_weight,
):
    row_total = hidden_states.shape[0]
    whole = lax.all_gather(hidden_states, "tp", axis=1, tiled=True)
    widened = whole.astype(jnp.float32)
    normed = (
        widened
        * lax.rsqrt(jnp.mean(widened * widened, axis=-1, keepdims=True) + EPS)
        * norm_gain[None, :]
    ).astype(jnp.bfloat16)
    slabs = (
        lax.all_gather(query_weight, "sp", axis=0, tiled=True),
        lax.all_gather(key_weight, "sp", axis=0, tiled=True),
        lax.all_gather(value_weight, "sp", axis=0, tiled=True),
        lax.all_gather(output_gate_weight, "sp", axis=0, tiled=True),
        lax.all_gather(unit_input_weight, "sp", axis=0, tiled=True),
        lax.all_gather(unit_gate_weight, "sp", axis=0, tiled=True),
    )
    summed = tuple((jnp.dot(normed, slab, preferred_element_type=jnp.float32) for slab in slabs))
    proj_q, proj_k, proj_v, proj_g, proj_a, proj_b = tuple(
        (part_sum.astype(jnp.bfloat16) for part_sum in summed)
    )
    head_count = proj_q.shape[1] // HEAD_DIM
    device = lax.axis_index("sp")
    positions = device * row_total + jnp.arange(row_total, dtype=jnp.int32)
    queries = rotate_at(proj_q.reshape(row_total, head_count, HEAD_DIM), positions)
    key_rows = rotate_at(proj_k.reshape(row_total, head_count, HEAD_DIM), positions)
    values = proj_v.reshape(row_total, head_count, HEAD_DIM)
    log_forward = jax.nn.log_sigmoid(decay_forward)
    log_backward = jax.nn.log_sigmoid(decay_backward)
    ahead_local, state_ahead = blockwise(
        to_blocks(queries), to_blocks(key_rows), to_blocks(values), log_forward, True
    )
    behind_local, state_behind = blockwise(
        to_blocks(queries[::-1]),
        to_blocks(key_rows[::-1]),
        to_blocks(values[::-1]),
        log_backward,
        False,
    )
    slabs = (
        lax.all_gather(state_ahead[None].astype(jnp.bfloat16), "sp", axis=0, tiled=True).astype(
            jnp.float32
        ),
        lax.all_gather(state_behind[None].astype(jnp.bfloat16), "sp", axis=0, tiled=True).astype(
            jnp.float32
        ),
    )
    source = jnp.arange(slabs[0].shape[0], dtype=jnp.int32)
    gap_ahead = device - 1 - source
    gap_behind = source - device - 1
    weight_ahead = jnp.where(
        gap_ahead[:, None] >= 0,
        jnp.exp(
            log_forward[None, :]
            * row_total
            * jnp.maximum(gap_ahead, 0).astype(jnp.float32)[:, None]
        ),
        0.0,
    )
    weight_behind = jnp.where(
        gap_behind[:, None] >= 0,
        jnp.exp(
            log_backward[None, :]
            * row_total
            * jnp.maximum(gap_behind, 0).astype(jnp.float32)[:, None]
        ),
        0.0,
    )
    enter_ahead = jnp.zeros_like(state_ahead) + jnp.einsum(
        "jh,jhde->hde", weight_ahead, slabs[0], precision=lax.Precision.HIGHEST
    )
    enter_behind = jnp.zeros_like(state_behind) + jnp.einsum(
        "jh,jhde->hde", weight_behind, slabs[1], precision=lax.Precision.HIGHEST
    )
    local_position = jnp.arange(row_total, dtype=jnp.float32)
    lift_ahead = jnp.exp(log_forward[None, :] * (local_position + 1.0)[:, None])
    lift_behind = jnp.exp(log_backward[None, :] * (row_total - local_position)[:, None])
    query_wide = queries.astype(jnp.float32)
    carried = jnp.einsum(
        "shd,hde->she",
        query_wide * lift_ahead[:, :, None],
        enter_ahead,
        precision=lax.Precision.HIGHEST,
    )
    carried = carried + jnp.einsum(
        "shd,hde->she",
        query_wide * lift_behind[:, :, None],
        enter_behind,
        precision=lax.Precision.HIGHEST,
    )
    retained = from_blocks(ahead_local) + from_blocks(behind_local)[::-1] + carried
    retention_rows = group_norm(retained, group_gain, group_bias, proj_g)
    unit = (proj_a.astype(jnp.float32) * jax.nn.sigmoid(proj_b.astype(jnp.float32))).astype(
        jnp.bfloat16
    )
    half_kernel = (KERNEL - 1) // 2
    padded = with_halo(unit, (("sp", 0),), half_kernel)
    filtered = jnp.broadcast_to(depth_bias[None, :], (row_total, unit.shape[1]))
    for offset in range(KERNEL):
        filtered = filtered + depth_kernel[offset][None, :] * padded[
            offset : offset + row_total
        ].astype(jnp.float32)
    row_sum, row_squares = lax.psum(
        (jnp.sum(filtered, axis=1), jnp.sum(filtered * filtered, axis=1)), "tp"
    )
    row_mean = (row_sum / CONV_WIDTH)[:, None]
    variance = (row_squares / CONV_WIDTH)[:, None] - row_mean * row_mean
    leveled = (filtered - row_mean) * lax.rsqrt(variance + EPS) * channel_gain[
        None, :
    ] + channel_bias[None, :]
    convolution_rows = jax.nn.silu(leveled).astype(jnp.bfloat16)
    retention_full, convolution_full = (
        lax.all_gather(retention_out_weight, "sp", axis=1, tiled=True),
        lax.all_gather(convolution_out_weight, "sp", axis=1, tiled=True),
    )
    return lax.psum_scatter(
        (
            jnp.dot(retention_rows, retention_full, preferred_element_type=jnp.float32)
            + jnp.dot(convolution_rows, convolution_full, preferred_element_type=jnp.float32)
        ).astype(jnp.bfloat16),
        "tp",
        scatter_dimension=0,
        tiled=True,
    )


def solution(mesh):
    n_sp, n_tp = mesh.shape["sp"], mesh.shape["tp"]
    fits = n_tp == 2 * CORES and n_sp % SIDES == 0
    fits = fits and n_sp // SIDES * n_tp * HEAD_DIM == CONV_WIDTH and n_sp // SIDES == n_tp
    placed = (
        P("sp", "tp"),
        P(),
        P("sp", "tp"),
        P("sp", "tp"),
        P("sp", "tp"),
        P("sp", "tp"),
        P("sp", "tp"),
        P("sp", "tp"),
        P("tp"),
        P("tp"),
        P("tp"),
        P("tp"),
        P(None, "tp"),
        P("tp"),
        P("tp"),
        P("tp"),
        P("tp", "sp"),
        P("tp", "sp"),
    )
    return jax.shard_map(
        fused if fits else shards_general,
        mesh=mesh, in_specs=placed, out_specs=P(("sp", "tp"), None), check_vma=False
    )
```

```python
import functools

import jax
import jax.numpy as jnp
import numpy as np
from jax import lax
from jax.experimental import pallas as pl
from jax.experimental.pallas import tpu as pltpu
from jax.sharding import PartitionSpec as P

HEAD_DIM = 128
CONV_WIDTH = 2048
KERNEL = 31

EPS = 1e-06
THETA = 10000.0
SIDES = 2
CORES = 2
BLOCK = 128
F32, BF16 = jnp.float32, jnp.bfloat16


class Copies:
    def __init__(self, sems):
        self.sems = sems
        self.used = 0
        self.pending = []

    def make(self, src, dst, arrived, device):
        copy = pltpu.make_async_remote_copy(
            src_ref=src,
            dst_ref=dst,
            send_sem=self.sems.at[self.used],
            recv_sem=arrived,
            device_id=device,
            device_id_type=pl.DeviceIdType.MESH,
        )
        self.used += 1
        return copy

    def send(self, src, dst, arrived, device, when=None):
        copy = self.make(src, dst, arrived, device)
        self.pending.append((copy, when))
        if when is None:
            copy.start()
        else:
            pl.when(when)(copy.start)

    def drain(self):
        for copy, when in self.pending:
            if when is None:
                copy.wait_send()
            else:
                pl.when(when)(copy.wait_send)


def fused_kernel(
    nz, half, n_tp, hid, gain, wq, wk, wv, wg, wa, wb, dec_f, dec_b, gg, gb, taps, dbias, cg, cb,
    wro, wco, table, out,
    xb, xg, ssq, wbuf, pj, ubuf, hx, fbuf, st, sr, tb, ef, eb, ts, tr, kr, dcol, dmat, mix,
    wo, ps, r1, s2, r2, ob, os_, oy,
    sends, lsem, rx_line, rx_y, rx_x, rx_c, rw_z, rw_y, r_wo, r_hx, r_stat, r_state, rm_c, rm_r,
    rs1, rs2, ro, roy,
):
    sp, tp = lax.axis_index("sp"), lax.axis_index("tp")
    z, y, x, c = sp // SIDES, sp % SIDES, tp // CORES, tp % CORES
    blk, feats = hid.shape
    depth = wq.shape[0]
    rows = nz * blk
    lanes = HEAD_DIM
    fine = out.shape[0]
    chunks = nz
    cols = SIDES * wro.shape[1]
    cp = Copies(sends)

    def dev(x_, y_, z_, c_):
        return (z_ * SIDES + y_, x_ * CORES + c_)

    other_x, other_y, other_c = dev(1 - x, y, z, c), dev(x, 1 - y, z, c), dev(x, y, z, 1 - c)
    here = dev(x, y, z, c)
    me = z * n_tp + tp
    group = nz * n_tp

    def arrive(dst, sem):
        pltpu.make_async_remote_copy(
            src_ref=dst, dst_ref=dst, send_sem=sem, recv_sem=sem,
            device_id=here, device_id_type=pl.DeviceIdType.MESH,
        ).wait_recv()

    def aligned(value, step):
        return pl.multiple_of(value, step)

    pairs = ((wa, wb), (wk, wv), (wq, wg))
    own_slot = jnp.where(z // SIDES == y, tp * nz + (z % SIDES) * SIDES + y, n_tp * nz + z % SIDES)
    local = [pltpu.make_async_copy(hid, xb.at[own_slot], lsem.at[0])]
    my_cols = pl.ds(aligned(z * lanes, lanes), lanes)
    my_depth = pl.ds(aligned(sp * depth, depth), depth)
    for p, pair in enumerate(pairs):
        for j, weight in enumerate(pair):
            local.append(
                pltpu.make_async_copy(
                    weight.at[:, my_cols],
                    wbuf.at[p, my_depth, pl.ds(j * lanes, lanes)],
                    lsem.at[1 + 2 * p + j],
                )
            )
    side_cols = pl.ds(aligned(y * (cols // SIDES), cols // SIDES), cols // SIDES)
    for k in range(nz):
        for j, weight in enumerate((wro, wco)):
            local.append(
                pltpu.make_async_copy(
                    weight.at[pl.ds(k * lanes, lanes)],
                    wo.at[pl.ds((2 * k + j) * lanes, lanes), side_cols],
                    lsem.at[7 + 2 * k + j],
                )
            )
    local.append(
        pltpu.make_async_copy(
            table.at[pl.ds(aligned(y * rows, rows), rows)], tb, lsem.at[7 + 2 * nz]
        )
    )
    for copy in local:
        copy.start()

    barrier = pltpu.get_barrier_semaphore()
    for k in range(1, group):
        idx = (me + k) % group
        pl.semaphore_signal(
            barrier, inc=1, device_id=((idx // n_tp) * SIDES + y, idx % n_tp),
            device_id_type=pl.DeviceIdType.MESH,
        )
    for k in range(nz):
        pl.semaphore_signal(
            barrier, inc=1, device_id=(k * SIDES + 1 - y, tp),
            device_id_type=pl.DeviceIdType.MESH,
        )
    pl.semaphore_wait(barrier, group - 1 + nz)

    def is_mine(zz):
        return zz // SIDES == y

    def line_slot(zz):
        return jnp.where(
            is_mine(zz), tp * nz + (zz % SIDES) * SIDES + y, n_tp * nz + zz % SIDES
        )

    def both(a, b):
        if a is None or b is None:
            return b if a is None else a
        return jnp.logical_and(a, b)

    def send_line(zz, step, when):
        slot = xb.at[line_slot(zz)]
        cp.send(slot, slot, rx_line.at[zz], dev(x, y, z + step, c), when)

    def share(b, when):
        slot = xb.at[tp * nz + b]
        cp.send(slot, slot, rx_x.at[b], other_x, when)
        cp.send(slot, slot, rx_c.at[b], other_c, when)

    def forward(zz, when=None):
        mine = is_mine(zz)
        cp.send(
            xb.at[n_tp * nz + zz % SIDES], xb.at[tp * nz + (zz % SIDES) * SIDES + y],
            rx_y.at[zz % SIDES], other_y, both(when, jnp.logical_not(mine)),
        )
        share((zz % SIDES) * SIDES + y, both(when, mine))

    at_end = jnp.logical_or(z == 0, z == nz - 1)
    inside = jnp.logical_not(at_end)

    def send_weights(p, when):
        for d in range(nz - 1, 0, -1):
            for zz, there in ((z - d, z >= d), (z + d, z + d < nz)):
                for j, weight in enumerate(pairs[p]):
                    cp.send(
                        weight.at[:, pl.ds(aligned(zz * lanes, lanes), lanes)],
                        wbuf.at[p, my_depth, pl.ds(j * lanes, lanes)],
                        rw_z.at[p, z], dev(x, y, zz, c), both(there, when),
                    )

    def weight_slice(p, zz, side):
        return wbuf.at[p, pl.ds(aligned((zz * SIDES + side) * depth, depth), depth)]

    def cross_weights(p, when=None):
        for d in range(1, nz):
            for zz, there in ((z - d, z >= d), (z + d, z + d < nz)):
                piece = weight_slice(p, zz, y)
                now = both(there, when)
                pl.when(now)(lambda piece=piece, zz=zz: arrive(piece, rw_z.at[p, zz]))
                cp.send(piece, piece, rw_y.at[p, zz], other_y, now)

    def await_weights(p):
        for zz in range(nz):
            arrive(weight_slice(p, zz, 1 - y), rw_y.at[p, zz])

    local[0].wait()
    send_line(z, 1, z < nz - 1)
    send_line(z, -1, z > 0)
    forward(z)

    def wo_piece(k, side):
        at = pl.ds(aligned(side * (cols // SIDES), cols // SIDES), cols // SIDES)
        return wo.at[pl.ds(k * 2 * lanes, 2 * lanes), at]

    def wo_send(k, when=None):
        piece = wo_piece(k, y)
        cp.send(piece, piece, r_wo.at[k], other_y, when)

    far = jnp.where(y == 0, z == nz - 1, z == 0)
    near = both(at_end, jnp.logical_not(far))

    def cross_own(p):
        local[1 + 2 * p].wait()
        local[2 + 2 * p].wait()
        piece = weight_slice(p, z, y)
        cp.send(piece, piece, rw_y.at[p, z], other_y)

    cross_own(0)
    for copy in local[7:-1]:
        copy.wait()
    for k in range(nz):
        wo_send(k, near)

    def y_arrivals(distance):
        for k in range(SIDES):
            zz = SIDES * y + k
            there = jnp.abs(z - zz) == distance
            b = k * SIDES + 1 - y
            pl.when(there)(lambda b=b, k=k: arrive(xb.at[tp * nz + b], rx_y.at[k]))
            share(b, there)

    for d in range(1, nz):
        low, high = z - d, z + d
        has_low, has_high = low >= 0, high < nz
        pl.when(has_low)(lambda low=low: arrive(xb.at[line_slot(low)], rx_line.at[low]))
        if d < nz - 1:
            send_line(low, 1, both(has_low, z < nz - 1))
        pl.when(has_high)(lambda high=high: arrive(xb.at[line_slot(high)], rx_line.at[high]))
        if d < nz - 1:
            send_line(high, -1, both(has_high, z > 0))
        forward(low, has_low)
        forward(high, has_high)
        if d == 1:
            cross_own(1)
        if d == 2:
            send_weights(0, None)
            cross_own(2)
            for k in range(nz):
                wo_send(k, far)
            send_weights(1, inside)
        if d == 3:
            send_weights(1, at_end)
            send_weights(2, None)
            wo_send(0, inside)
        y_arrivals(d - 1)
    cross_weights(0, far)
    y_arrivals(nz - 1)
    pad = 16
    edge_rows = xb.at[n_tp * nz + y, pl.ds(aligned(y * (blk - pad), pad), pad)]
    for k in range(1, n_tp):
        cp.send(edge_rows, hx.at[tp], r_hx.at[tp], (sp, (tp + k) % n_tp))

    def pick(ref):
        here_lane = lax.broadcasted_iota(jnp.int32, ref.shape, 1) == z
        v = jnp.sum(jnp.where(here_lane, ref[...], 0.0), axis=1, keepdims=True)
        e = jnp.exp(-jnp.abs(v))
        small = e * (1.0 - e * (0.5 - e * (1.0 / 3.0 - e * 0.25)))
        return jnp.minimum(v, 0.0) - jnp.where(e < 1e-2, small, jnp.log(1.0 + e))

    log_f, log_b = pick(dec_f), pick(dec_b)
    index = lax.broadcasted_iota(jnp.int32, (blk, lanes), 0).astype(F32)
    dcol[0] = jnp.exp(log_f * (blk - 1.0 - index))
    dcol[1] = jnp.exp(log_b * index)
    dcol[2] = jnp.exp(log_f * (index + 1.0))
    dcol[3] = jnp.exp(log_b * (blk - index))
    across = lax.broadcasted_iota(jnp.int32, (blk, blk), 0) - lax.broadcasted_iota(
        jnp.int32, (blk, blk), 1
    )
    away = across.astype(F32)
    dmat[...] = jnp.exp(jnp.where(across >= 0, log_f * away, -log_b * away))
    leap_f, leap_b = jnp.exp(log_f * float(blk)), jnp.exp(log_b * float(blk))

    def gather_squares(q, first):
        at = pl.ds(aligned(q * feats, feats), feats)

        def strip(i, carry):
            r = pl.ds(aligned(i * 16, 16), 16)
            v = xb[q * nz + i // (blk // 16), pl.ds(aligned((i % (blk // 16)) * 16, 16), 16)]
            v = v.astype(F32)
            xg[r, at] = (v * gain[:, at]).astype(BF16)
            w = v * v
            s = w[:, :lanes]
            for k in range(1, feats // lanes):
                s = s + w[:, k * lanes : (k + 1) * lanes]
            ssq[r] = s if first else ssq[r] + s
            return carry

        lax.fori_loop(0, rows // 16, strip, 0)

    width = n_tp * feats

    def finish(i, carry):
        r = pl.ds(aligned(i * 128, 128), 128)
        total = jnp.sum(ssq[r], axis=1, keepdims=True)
        ssq[r] = jnp.broadcast_to(lax.rsqrt(total / width + EPS), (128, lanes))
        return carry

    def project(p):
        tall = 2 * blk

        def body(i, carry):
            r = pl.ds(aligned(i * tall, tall), tall)
            scale = ssq[r]
            acc = jnp.dot(xg[r], wbuf[p], preferred_element_type=F32)
            pj[p, r, pl.ds(0, lanes)] = (acc[:, :lanes] * scale).astype(BF16)
            pj[p, r, pl.ds(lanes, lanes)] = (acc[:, lanes:] * scale).astype(BF16)
            return carry

        lax.fori_loop(0, rows // tall, body, 0)

    def edge_unit():
        hx[tp] = edge_rows[...]
        r = pl.ds(rows, pad)
        total = jnp.zeros((pad, 1), F32)
        for q in range(n_tp):
            at = pl.ds(q * feats, feats)
            v = hx[q].astype(F32)
            xg[r, at] = (v * gain[:, at]).astype(BF16)
            total = total + jnp.sum(v * v, axis=1, keepdims=True)
        scale = lax.rsqrt(total / width + EPS)
        acc = jnp.dot(xg[r], wbuf[0], preferred_element_type=F32) * scale
        a = acc[:, :lanes].astype(BF16).astype(F32)
        b = acc[:, lanes:].astype(BF16).astype(F32)
        unit = (a * jax.nn.sigmoid(b)).astype(BF16).astype(F32)
        ubuf[pl.ds(0, pad)] = jnp.where(y == 1, unit, 0.0)
        ubuf[pl.ds(pad + rows, pad)] = jnp.where(y == 0, unit, 0.0)

    def gate(i, carry):
        r = aligned(i * 128, 128)
        a = pj[0, pl.ds(r, 128), pl.ds(0, lanes)].astype(F32)
        b = pj[0, pl.ds(r, 128), pl.ds(lanes, lanes)].astype(F32)
        ubuf[pl.ds(aligned(r + pad, 16), 128)] = (a * jax.nn.sigmoid(b)).astype(BF16).astype(F32)
        return carry

    wts = taps[:, my_cols]
    bias = dbias[:, my_cols]
    count = rows // 128
    reach = (KERNEL - 1) // 2

    def convolve(i, carry):
        block = i
        for part in range(2):
            r = aligned(block * 128 + part * 64, 64)
            acc = jnp.broadcast_to(bias, (64, lanes))
            for t in range(KERNEL):
                acc = acc + wts[t : t + 1] * ubuf[pl.ds(r + (pad - reach + t), 64)]
            fbuf[pl.ds(r, 64)] = acc
        turned = fbuf[pl.ds(aligned(block * 128, 128), 128)].T
        st[pl.ds(block, 1)] = jnp.sum(turned, axis=0, keepdims=True)
        st[pl.ds(count + block, 1)] = jnp.sum(turned * turned, axis=0, keepdims=True)
        return carry

    def mix_part(zz, r, conv):
        start = zz * 2 * lanes + (lanes if conv else 0)
        return mix.at[r, pl.ds(aligned(start, lanes), lanes)]

    def mix_send(zz, r, conv, sem, step, when):
        part = mix_part(zz, r, conv)
        cp.send(part, part, sem, dev(x, y, z + step, c), when)

    def mix_hop(d, r, conv, sems):
        low, high = z - d, z + d
        has_low, has_high = low >= 0, high < nz
        pl.when(has_low)(lambda: arrive(mix_part(low, r, conv), sems.at[low]))
        if d < nz - 1:
            mix_send(low, r, conv, sems.at[low], 1, both(has_low, z < nz - 1))
        pl.when(has_high)(lambda: arrive(mix_part(high, r, conv), sems.at[high]))
        if d < nz - 1:
            mix_send(high, r, conv, sems.at[high], -1, both(has_high, z > 0))

    first_half = lax.broadcasted_iota(jnp.int32, (blk, lanes), 1) < lanes // 2

    def turn(v, r):
        t = tb[r]
        rolled = pltpu.roll(t, lanes // 2, 1)
        cosine = jnp.where(first_half, t, rolled)
        sine = jnp.where(first_half, -rolled, t)
        return (v * cosine + pltpu.roll(v, lanes // 2, 1) * sine).astype(BF16)

    def states(i, carry):
        r = pl.ds(aligned(i * blk, blk), blk)
        keys = turn(pj[1, r, pl.ds(0, lanes)].astype(F32), r)
        kr[r] = keys
        wide = keys.astype(F32)
        both_ways = jnp.concatenate(
            [(wide * dcol[0]).astype(BF16), (wide * dcol[1]).astype(BF16)], axis=1
        )
        state = lax.dot_general(
            both_ways, pj[1, r, pl.ds(lanes, lanes)], (((0,), (0,)), ((), ())),
            preferred_element_type=F32,
        )
        ef[i] = state[:lanes]
        eb[i] = state[lanes:]
        return carry

    cross_weights(0, jnp.logical_not(far))
    cross_weights(1, far)
    far_q = dev(1 - x, y, z, c)[1]
    for b in range(nz):
        slot = xb.at[far_q * nz + b]
        arrive(slot, rx_x.at[b])
        cp.send(slot, slot, rx_c.at[nz + b], other_c)
    gather_squares(tp, True)
    gather_squares(far_q, False)
    for k, q in enumerate((dev(x, y, z, 1 - c)[1], dev(1 - x, y, z, 1 - c)[1])):
        for b in range(nz):
            arrive(xb.at[q * nz + b], rx_c.at[k * nz + b])
        gather_squares(q, False)

    lax.fori_loop(0, rows // 128, finish, 0)

    for k in range(1, n_tp):
        peer = (tp + k) % n_tp
        arrive(hx.at[peer], r_hx.at[peer])
    await_weights(0)
    project(0)
    edge_unit()
    lax.fori_loop(0, rows // 128, gate, 0)
    lax.fori_loop(0, count, convolve, 0)
    for k in range(1, group):
        idx = (me + k) % group
        cp.send(
            st, sr.at[me], r_stat.at[me], ((idx // n_tp) * SIDES + y, idx % n_tp)
        )
    sr[me] = st[...]
    cross_weights(1, jnp.logical_not(far))
    cross_weights(2)
    for k in range(1, group):
        idx = (me + k) % group
        arrive(sr.at[idx], r_stat.at[idx])
    sums = sr[0]
    for k in range(1, group):
        sums = sums + sr[k]
    st_mean = sums[:count] / CONV_WIDTH
    st_scale = lax.rsqrt(sums[count:] / CONV_WIDTH - st_mean * st_mean + EPS)
    conv_cols = pl.ds(aligned(z * 2 * lanes + lanes, lanes), lanes)
    ret_cols = pl.ds(aligned(z * 2 * lanes, lanes), lanes)
    gain_c, bias_c = cg[:, my_cols], cb[:, my_cols]
    for i in range(count):
        r = pl.ds(i * 128, 128)
        mean = jnp.broadcast_to(st_mean[i : i + 1], (128, lanes)).T
        scale = jnp.broadcast_to(st_scale[i : i + 1], (128, lanes)).T
        level = (fbuf[r] - mean) * scale * gain_c + bias_c
        mix[r, conv_cols] = (level * jax.nn.sigmoid(level)).astype(BF16)

    every = pl.ds(0, rows)
    mix_send(z, every, True, rm_c.at[z], 1, z < nz - 1)
    mix_send(z, every, True, rm_c.at[z], -1, z > 0)

    await_weights(1)
    project(1)
    local[-1].wait()
    lax.fori_loop(0, chunks, states, 0)
    run = ef[0]
    ef[0] = jnp.zeros_like(run)
    for i in range(1, chunks):
        own = ef[i]
        ef[i] = run
        run = run * leap_f + own
    back = eb[chunks - 1]
    eb[chunks - 1] = jnp.zeros_like(back)
    for i in range(chunks - 2, -1, -1):
        own = eb[i]
        eb[i] = back
        back = back * leap_b + own
    ts[...] = jnp.where(y == 0, run, back).astype(BF16)
    cp.send(ts, tr, r_state, other_y)

    for k in range(1, nz):
        wo_send(k, inside)
    mix_hop(1, every, True, rm_c)
    await_weights(2)
    project(2)
    arrive(tr, r_state)
    entering = tr[...].astype(F32)
    entering_f = jnp.where(y == 1, entering, 0.0)
    entering_b = jnp.where(y == 0, entering, 0.0)
    for i in range(chunks):
        ef[i] = ef[i] + entering_f
        entering_f = entering_f * leap_f
    for i in range(chunks - 1, -1, -1):
        eb[i] = eb[i] + entering_b
        entering_b = entering_b * leap_b
    mix_hop(2, every, True, rm_c)
    gain_r, bias_r = gg[:, my_cols], gb[:, my_cols]

    def retain(i, carry):
        r = pl.ds(aligned(i * blk, blk), blk)
        queries = turn(pj[2, r, pl.ds(0, lanes)].astype(F32), r)
        keys, values = kr[r], pj[1, r, pl.ds(lanes, lanes)]
        scores = lax.dot_general(
            queries, keys, (((1,), (1,)), ((), ())), preferred_element_type=F32
        )
        scores = (scores * dmat[...]).astype(BF16)
        inner = jnp.dot(scores, values, preferred_element_type=F32)
        enter = jnp.concatenate([ef[i], eb[i]], axis=1).astype(BF16)
        carried = jnp.dot(queries, enter, preferred_element_type=F32)
        retained = inner + carried[:, :lanes] * dcol[2] + carried[:, lanes:] * dcol[3]
        mean = jnp.mean(retained, axis=-1, keepdims=True)
        centered = retained - mean
        spread = jnp.mean(centered * centered, axis=-1, keepdims=True)
        scaled = centered * lax.rsqrt(spread + EPS) * gain_r + bias_r
        g = pj[2, r, pl.ds(lanes, lanes)].astype(F32)
        mix[r, ret_cols] = (g * jax.nn.sigmoid(g) * scaled).astype(BF16)
        return carry

    spans = [pl.ds(i * blk, blk) for i in range(chunks)]

    def ret_send(i):
        mix_send(z, spans[i], False, rm_r.at[i, z], 1, z < nz - 1)
        mix_send(z, spans[i], False, rm_r.at[i, z], -1, z > 0)

    def ret_hop(d, i):
        mix_hop(d, spans[i], False, rm_r.at[i])

    for i in range(chunks):
        lax.fori_loop(i, i + 1, retain, 0)
        if i < 2:
            ret_send(i)
    mix_hop(3, every, True, rm_c)
    for k in range(nz):
        piece = wo_piece(k, 1 - y)
        arrive(piece, r_wo.at[k])
    def multiply(i):
        acc = jnp.dot(mix[spans[i]], wo[...], preferred_element_type=F32)
        for t in range(n_tp):
            ps[i, t % CORES, t // CORES] = acc[t * fine : (t + 1) * fine].astype(BF16)
        cp.send(ps.at[i, 1 - c], r1.at[i], rs1.at[i], other_c)

    def add_cores(i):
        arrive(r1.at[i], rs1.at[i])
        s2[i] = (ps[i, c, 1 - x].astype(F32) + r1[i, 1 - x].astype(F32)).astype(BF16)
        cp.send(s2.at[i], r2.at[i], rs2.at[i], other_x)

    def add_far(i):
        arrive(r2.at[i], rs2.at[i])
        total = ps[i, c, x].astype(F32) + r1[i, x].astype(F32) + r2[i].astype(F32)
        os_[i] = total.astype(BF16)
        same_side = y == i % SIDES
        z_to = SIDES * y + i // SIDES
        apart = jnp.logical_and(same_side, z_to != z)
        cp.send(os_.at[i], ob.at[z], ro.at[z], dev(x, y, z_to, c), apart)

        @pl.when(jnp.logical_and(same_side, z_to == z))
        def _():
            ob[z] = os_[i]

        cp.send(
            os_.at[i], oy.at[i // SIDES], roy.at[i // SIDES], other_y, jnp.logical_not(same_side)
        )

    def relay(k):
        arrive(oy.at[k], roy.at[k])
        z_to = SIDES * (1 - y) + k
        apart = z_to != z
        cp.send(oy.at[k], ob.at[z], ro.at[z], dev(x, y, z_to, c), apart)

        @pl.when(z_to == z)
        def _():
            ob[z] = oy[k]

    ret_hop(1, 0)
    ret_send(2)
    ret_hop(1, 1)
    ret_hop(2, 0)
    ret_send(3)
    ret_hop(1, 2)
    ret_hop(2, 1)
    ret_hop(3, 0)
    multiply(0)
    ret_hop(1, 3)
    ret_hop(2, 2)
    ret_hop(3, 1)
    multiply(1)
    add_cores(0)
    ret_hop(2, 3)
    ret_hop(3, 2)
    multiply(2)
    add_cores(1)
    add_far(0)
    ret_hop(3, 3)
    multiply(3)
    add_cores(2)
    add_far(1)
    add_cores(3)
    add_far(2)
    relay(0)
    add_far(3)
    relay(1)
    for zz in range(nz):
        @pl.when(zz != z)
        def _():
            arrive(ob.at[zz], ro.at[zz])

        out[:, pl.ds(zz * cols, cols)] = ob[zz]
    cp.drain()


def fused(
    hidden_states, norm_gain, query_weight, key_weight, value_weight, output_gate_weight,
    unit_input_weight, unit_gate_weight, decay_forward, decay_backward, group_gain, group_bias,
    depth_kernel, depth_bias, channel_gain, channel_bias, retention_out_weight,
    convolution_out_weight,
):
    n_sp, n_tp = lax.axis_size("sp"), lax.axis_size("tp")
    nz = n_sp // SIDES
    blk, feats = hidden_states.shape
    depth = query_weight.shape[0]
    rows = nz * blk
    lanes = HEAD_DIM
    cols = SIDES * retention_out_weight.shape[1]
    fine = blk // n_tp
    half_dim = lanes // 2
    inverse = np.float32(THETA) ** (-np.arange(half_dim, dtype=np.float32) / np.float32(half_dim))
    angles = np.arange(SIDES * rows, dtype=np.float32)[:, None] * inverse.astype(np.float32)[None]
    table = np.concatenate([np.cos(angles.astype(np.float64)), np.sin(angles.astype(np.float64))], 1)
    table = jnp.asarray(table.astype(np.float32))
    count = rows // 128

    def row(v):
        return v.reshape(1, v.shape[0])

    any_, vmem = pl.BlockSpec(memory_space=pl.ANY), pl.BlockSpec(memory_space=pltpu.VMEM)
    dma = pltpu.SemaphoreType.DMA
    group = nz * n_tp
    return pl.pallas_call(
        functools.partial(fused_kernel, nz, SIDES, n_tp),
        out_shape=jax.ShapeDtypeStruct((fine, nz * cols), BF16),
        in_specs=[any_, vmem] + [any_] * 6 + [vmem] * 8 + [any_] * 3,
        out_specs=vmem,
        scratch_shapes=[
            pltpu.VMEM((n_tp * nz + SIDES, blk, feats), BF16),
            pltpu.VMEM((rows + 16, n_tp * feats), BF16),
            pltpu.VMEM((rows, lanes), F32),
            pltpu.VMEM((3, n_sp * depth, 2 * lanes), BF16),
            pltpu.VMEM((3, rows, 2 * lanes), BF16),
            pltpu.VMEM((rows + 32, lanes), F32),
            pltpu.VMEM((n_tp, 16, feats), BF16),
            pltpu.VMEM((rows, lanes), F32),
            pltpu.VMEM((2 * count, lanes), F32),
            pltpu.VMEM((group, 2 * count, lanes), F32),
            pltpu.VMEM((rows, lanes), F32),
            pltpu.VMEM((nz, lanes, lanes), F32),
            pltpu.VMEM((nz, lanes, lanes), F32),
            pltpu.VMEM((lanes, lanes), BF16),
            pltpu.VMEM((lanes, lanes), BF16),
            pltpu.VMEM((rows, lanes), BF16),
            pltpu.VMEM((4, blk, lanes), F32),
            pltpu.VMEM((blk, blk), F32),
            pltpu.VMEM((rows, nz * 2 * lanes), BF16),
            pltpu.VMEM((nz * 2 * lanes, cols), BF16),
            pltpu.VMEM((nz, CORES, n_tp // CORES, fine, cols), BF16),
            pltpu.VMEM((nz, n_tp // CORES, fine, cols), BF16),
            pltpu.VMEM((nz, fine, cols), BF16),
            pltpu.VMEM((nz, fine, cols), BF16),
            pltpu.VMEM((nz, fine, cols), BF16),
            pltpu.VMEM((nz, fine, cols), BF16),
            pltpu.VMEM((SIDES, fine, cols), BF16),
            dma((300,)),
            dma((8 + 2 * nz,)),
            dma((nz,)), dma((SIDES,)), dma((nz,)), dma((2 * nz,)),
            dma((3, nz)), dma((3, nz)),
            dma((nz,)), dma((n_tp,)), dma((group,)), dma,
            dma((nz,)), dma((nz, nz)),
            dma((nz,)), dma((nz,)), dma((nz,)), dma((SIDES,)),
        ],
        compiler_params=pltpu.CompilerParams(
            collective_id=0, has_side_effects=True, vmem_limit_bytes=60 * 1024 * 1024
        ),
    )(
        hidden_states, row(norm_gain), query_weight, key_weight, value_weight, output_gate_weight,
        unit_input_weight, unit_gate_weight, row(decay_forward), row(decay_backward),
        row(group_gain), row(group_bias), depth_kernel, row(depth_bias), row(channel_gain),
        row(channel_bias), retention_out_weight, convolution_out_weight, table,
    )


def with_halo(cells, sides, width):
    for axis, dim in sides:
        count = lax.axis_size(axis)
        ends = count - 1
        head = lax.slice_in_dim(cells, 0, width, axis=dim)
        tail = lax.slice_in_dim(cells, cells.shape[dim] - width, cells.shape[dim], axis=dim)
        cells = jnp.concatenate(
            [
                lax.ppermute(tail, axis, [(i, (i + 1) % count) for i in range(ends)]),
                cells,
                lax.ppermute(head, axis, [((i + 1) % count, i) for i in range(ends)]),
            ],
            axis=dim,
        )
    return cells


def rotate_at(rows, positions):
    half_dim = rows.shape[-1] // 2
    inverse = THETA ** (-jnp.arange(half_dim, dtype=jnp.float32) / half_dim)
    angles = positions.astype(jnp.float32)[:, None] * inverse[None, :]
    cosine = jnp.cos(angles)[:, None, :]
    sine = jnp.sin(angles)[:, None, :]
    widened = rows.astype(jnp.float32)
    first_half = widened[..., :half_dim]
    second_half = widened[..., half_dim:]
    turned = jnp.concatenate(
        [first_half * cosine - second_half * sine, second_half * cosine + first_half * sine],
        axis=-1,
    )
    return turned.astype(jnp.bfloat16)


def to_blocks(rows):
    return rows.reshape(rows.shape[0] // BLOCK, BLOCK, rows.shape[1], rows.shape[2]).transpose(
        2, 0, 1, 3
    )


def from_blocks(blocks):
    return blocks.transpose(1, 2, 0, 3).reshape(
        blocks.shape[1] * blocks.shape[2], blocks.shape[0], blocks.shape[3]
    )


def blockwise(queries, key_rows, values, log_decay, include_diag):
    block_len = queries.shape[2]
    position = jnp.arange(block_len, dtype=jnp.float32)
    distance = position[:, None] - position[None, :]
    allowed = distance >= 0 if include_diag else distance > 0
    inside = jnp.where(
        allowed[None], jnp.exp(log_decay[:, None, None] * jnp.maximum(distance, 0.0)[None]), 0.0
    )
    query_wide = queries.astype(jnp.float32)
    key_wide = key_rows.astype(jnp.float32)
    value_wide = values.astype(jnp.float32)
    scores = (
        jnp.einsum("hnqd,hnkd->hnqk", query_wide, key_wide, precision=lax.Precision.HIGHEST)
        * inside[:, None]
    )
    inner_part = jnp.einsum("hnqk,hnkd->hnqd", scores, value_wide, precision=lax.Precision.HIGHEST)
    toward_end = jnp.exp(log_decay[:, None] * (block_len - 1.0 - position)[None])
    block_states = jnp.einsum(
        "hnkd,hnke->hnde",
        key_wide * toward_end[:, None, :, None],
        value_wide,
        precision=lax.Precision.HIGHEST,
    )
    block_decay = jnp.exp(log_decay * block_len)[:, None, None]

    def advance(state_now, block_state):
        return (block_decay * state_now + block_state, state_now)

    initial = jnp.zeros(
        (block_states.shape[0], block_states.shape[2], block_states.shape[3]), jnp.float32
    )
    final_state, earlier = lax.scan(advance, initial, jnp.moveaxis(block_states, 1, 0))
    earlier = jnp.moveaxis(earlier, 0, 1)
    from_start = jnp.exp(log_decay[:, None] * (position + 1.0)[None])
    cross_part = jnp.einsum(
        "hnqd,hnde->hnqe",
        query_wide * from_start[:, None, :, None],
        earlier,
        precision=lax.Precision.HIGHEST,
    )
    return (inner_part + cross_part, final_state)


def group_norm(retained, group_gain, group_bias, gate_rows):
    row_mean = jnp.mean(retained, axis=-1, keepdims=True)
    centered = retained - row_mean
    variance = jnp.mean(centered * centered, axis=-1, keepdims=True)
    scaled = (centered * lax.rsqrt(variance + EPS)).reshape(retained.shape[0], -1)
    scaled = scaled * group_gain[None, :] + group_bias[None, :]
    return (jax.nn.silu(gate_rows.astype(jnp.float32)) * scaled).astype(jnp.bfloat16)


def shards_general(
    hidden_states,
    norm_gain,
    query_weight,
    key_weight,
    value_weight,
    output_gate_weight,
    unit_input_weight,
    unit_gate_weight,
    decay_forward,
    decay_backward,
    group_gain,
    group_bias,
    depth_kernel,
    depth_bias,
    channel_gain,
    channel_bias,
    retention_out_weight,
    convolution_out_weight,
):
    row_total = hidden_states.shape[0]
    whole = lax.all_gather(hidden_states, "tp", axis=1, tiled=True)
    widened = whole.astype(jnp.float32)
    normed = (
        widened
        * lax.rsqrt(jnp.mean(widened * widened, axis=-1, keepdims=True) + EPS)
        * norm_gain[None, :]
    ).astype(jnp.bfloat16)
    slabs = (
        lax.all_gather(query_weight, "sp", axis=0, tiled=True),
        lax.all_gather(key_weight, "sp", axis=0, tiled=True),
        lax.all_gather(value_weight, "sp", axis=0, tiled=True),
        lax.all_gather(output_gate_weight, "sp", axis=0, tiled=True),
        lax.all_gather(unit_input_weight, "sp", axis=0, tiled=True),
        lax.all_gather(unit_gate_weight, "sp", axis=0, tiled=True),
    )
    summed = tuple((jnp.dot(normed, slab, preferred_element_type=jnp.float32) for slab in slabs))
    proj_q, proj_k, proj_v, proj_g, proj_a, proj_b = tuple(
        (part_sum.astype(jnp.bfloat16) for part_sum in summed)
    )
    head_count = proj_q.shape[1] // HEAD_DIM
    device = lax.axis_index("sp")
    positions = device * row_total + jnp.arange(row_total, dtype=jnp.int32)
    queries = rotate_at(proj_q.reshape(row_total, head_count, HEAD_DIM), positions)
    key_rows = rotate_at(proj_k.reshape(row_total, head_count, HEAD_DIM), positions)
    values = proj_v.reshape(row_total, head_count, HEAD_DIM)
    log_forward = jax.nn.log_sigmoid(decay_forward)
    log_backward = jax.nn.log_sigmoid(decay_backward)
    ahead_local, state_ahead = blockwise(
        to_blocks(queries), to_blocks(key_rows), to_blocks(values), log_forward, True
    )
    behind_local, state_behind = blockwise(
        to_blocks(queries[::-1]),
        to_blocks(key_rows[::-1]),
        to_blocks(values[::-1]),
        log_backward,
        False,
    )
    slabs = (
        lax.all_gather(state_ahead[None].astype(jnp.bfloat16), "sp", axis=0, tiled=True).astype(
            jnp.float32
        ),
        lax.all_gather(state_behind[None].astype(jnp.bfloat16), "sp", axis=0, tiled=True).astype(
            jnp.float32
        ),
    )
    source = jnp.arange(slabs[0].shape[0], dtype=jnp.int32)
    gap_ahead = device - 1 - source
    gap_behind = source - device - 1
    weight_ahead = jnp.where(
        gap_ahead[:, None] >= 0,
        jnp.exp(
            log_forward[None, :]
            * row_total
            * jnp.maximum(gap_ahead, 0).astype(jnp.float32)[:, None]
        ),
        0.0,
    )
    weight_behind = jnp.where(
        gap_behind[:, None] >= 0,
        jnp.exp(
            log_backward[None, :]
            * row_total
            * jnp.maximum(gap_behind, 0).astype(jnp.float32)[:, None]
        ),
        0.0,
    )
    enter_ahead = jnp.zeros_like(state_ahead) + jnp.einsum(
        "jh,jhde->hde", weight_ahead, slabs[0], precision=lax.Precision.HIGHEST
    )
    enter_behind = jnp.zeros_like(state_behind) + jnp.einsum(
        "jh,jhde->hde", weight_behind, slabs[1], precision=lax.Precision.HIGHEST
    )
    local_position = jnp.arange(row_total, dtype=jnp.float32)
    lift_ahead = jnp.exp(log_forward[None, :] * (local_position + 1.0)[:, None])
    lift_behind = jnp.exp(log_backward[None, :] * (row_total - local_position)[:, None])
    query_wide = queries.astype(jnp.float32)
    carried = jnp.einsum(
        "shd,hde->she",
        query_wide * lift_ahead[:, :, None],
        enter_ahead,
        precision=lax.Precision.HIGHEST,
    )
    carried = carried + jnp.einsum(
        "shd,hde->she",
        query_wide * lift_behind[:, :, None],
        enter_behind,
        precision=lax.Precision.HIGHEST,
    )
    retained = from_blocks(ahead_local) + from_blocks(behind_local)[::-1] + carried
    retention_rows = group_norm(retained, group_gain, group_bias, proj_g)
    unit = (proj_a.astype(jnp.float32) * jax.nn.sigmoid(proj_b.astype(jnp.float32))).astype(
        jnp.bfloat16
    )
    half_kernel = (KERNEL - 1) // 2
    padded = with_halo(unit, (("sp", 0),), half_kernel)
    filtered = jnp.broadcast_to(depth_bias[None, :], (row_total, unit.shape[1]))
    for offset in range(KERNEL):
        filtered = filtered + depth_kernel[offset][None, :] * padded[
            offset : offset + row_total
        ].astype(jnp.float32)
    row_sum, row_squares = lax.psum(
        (jnp.sum(filtered, axis=1), jnp.sum(filtered * filtered, axis=1)), "tp"
    )
    row_mean = (row_sum / CONV_WIDTH)[:, None]
    variance = (row_squares / CONV_WIDTH)[:, None] - row_mean * row_mean
    leveled = (filtered - row_mean) * lax.rsqrt(variance + EPS) * channel_gain[
        None, :
    ] + channel_bias[None, :]
    convolution_rows = jax.nn.silu(leveled).astype(jnp.bfloat16)
    retention_full, convolution_full = (
        lax.all_gather(retention_out_weight, "sp", axis=1, tiled=True),
        lax.all_gather(convolution_out_weight, "sp", axis=1, tiled=True),
    )
    return lax.psum_scatter(
        (
            jnp.dot(retention_rows, retention_full, preferred_element_type=jnp.float32)
            + jnp.dot(convolution_rows, convolution_full, preferred_element_type=jnp.float32)
        ).astype(jnp.bfloat16),
        "tp",
        scatter_dimension=0,
        tiled=True,
    )


def solution(mesh):
    n_sp, n_tp = mesh.shape["sp"], mesh.shape["tp"]
    fits = n_tp == 2 * CORES and n_sp % SIDES == 0
    fits = fits and n_sp // SIDES * n_tp * HEAD_DIM == CONV_WIDTH and n_sp // SIDES == n_tp
    placed = (
        P("sp", "tp"),
        P(),
        P("sp", "tp"),
        P("sp", "tp"),
        P("sp", "tp"),
        P("sp", "tp"),
        P("sp", "tp"),
        P("sp", "tp"),
        P("tp"),
        P("tp"),
        P("tp"),
        P("tp"),
        P(None, "tp"),
        P("tp"),
        P("tp"),
        P("tp"),
        P("tp", "sp"),
        P("tp", "sp"),
    )
    return jax.shard_map(
        fused if fits else shards_general,
        mesh=mesh, in_specs=placed, out_specs=P(("sp", "tp"), None), check_vma=False
    )
```

```python
import functools

import jax
import jax.numpy as jnp
import numpy as np
from jax import lax
from jax.experimental import pallas as pl
from jax.experimental.pallas import tpu as pltpu
from jax.sharding import PartitionSpec as P

HEAD_DIM = 128
CONV_WIDTH = 2048
KERNEL = 31

EPS = 1e-06
THETA = 10000.0
SIDES = 2
CORES = 2
BLOCK = 128
F32, BF16 = jnp.float32, jnp.bfloat16


class Copies:
    def __init__(self, sems):
        self.sems = sems
        self.used = 0
        self.pending = []

    def make(self, src, dst, arrived, device):
        copy = pltpu.make_async_remote_copy(
            src_ref=src,
            dst_ref=dst,
            send_sem=self.sems.at[self.used],
            recv_sem=arrived,
            device_id=device,
            device_id_type=pl.DeviceIdType.MESH,
        )
        self.used += 1
        return copy

    def send(self, src, dst, arrived, device, when=None):
        copy = self.make(src, dst, arrived, device)
        self.pending.append((copy, when))
        if when is None:
            copy.start()
        else:
            pl.when(when)(copy.start)

    def drain(self):
        for copy, when in self.pending:
            if when is None:
                copy.wait_send()
            else:
                pl.when(when)(copy.wait_send)


def fused_kernel(
    nz, n_tp, hid, gain, wq, wk, wv, wg, wa, wb, dec_f, dec_b, gg, gb, taps, dbias, cg, cb,
    wro, wco, table, out,
    xb, xg, ssq, sqs, sqr, sqt, scl, turned_edge, wbuf, own, pso, pre, pj, es, er, ubuf, fbuf,
    st, sr, tb, ef, eb, ts, tr, kr, dcol, dmat, mix, wo, ps, r1, s2, r2, ob, os_, oy,
    sends, lsem, rx_y, rx_line, rx_x, rx_c, rw, r_wo, r_sq, r_p, r_e, r_stat, r_state, rm_c,
    rm_r, rs1, rs2, ro, roy,
):
    sp, tp = lax.axis_index("sp"), lax.axis_index("tp")
    z, y, x, c = sp // SIDES, sp % SIDES, tp // CORES, tp % CORES
    n_sp = nz * SIDES
    blk, feats = hid.shape
    part = feats // SIDES
    depth = wq.shape[0]
    rows = nz * blk
    lanes = HEAD_DIM
    fine = out.shape[0]
    chunks = nz
    count = rows // 128
    cols = SIDES * wro.shape[1]
    cp = Copies(sends)

    def dev(x_, y_, z_, c_):
        return (z_ * SIDES + y_, x_ * CORES + c_)

    other_x, other_y, other_c = dev(1 - x, y, z, c), dev(x, 1 - y, z, c), dev(x, y, z, 1 - c)
    here = dev(x, y, z, c)
    me = z * n_tp + tp
    group = nz * n_tp

    def arrive(dst, sem):
        pltpu.make_async_remote_copy(
            src_ref=dst, dst_ref=dst, send_sem=sem, recv_sem=sem,
            device_id=here, device_id_type=pl.DeviceIdType.MESH,
        ).wait_recv()

    def aligned(value, step):
        return pl.multiple_of(value, step)

    def both(a, b):
        if a is None or b is None:
            return b if a is None else a
        return jnp.logical_and(a, b)

    pairs = ((wa, wb), (wk, wv), (wq, wg))
    my_cols = pl.ds(aligned(z * lanes, lanes), lanes)
    my_depth = pl.ds(aligned(z * depth, depth), depth)
    near_part = hid.at[:, pl.ds(aligned(y * part, part), part)]
    far_part = hid.at[:, pl.ds(aligned((1 - y) * part, part), part)]
    local = [pltpu.make_async_copy(near_part, xb.at[tp, sp], lsem.at[0])]
    for p, pair in enumerate(pairs):
        for j, weight in enumerate(pair):
            local.append(
                pltpu.make_async_copy(
                    weight.at[:, my_cols],
                    wbuf.at[p, my_depth, pl.ds(j * lanes, lanes)],
                    lsem.at[1 + 2 * p + j],
                )
            )
    side_cols = pl.ds(aligned(y * (cols // SIDES), cols // SIDES), cols // SIDES)
    far_cols = pl.ds(aligned((1 - y) * (cols // SIDES), cols // SIDES), cols // SIDES)
    for k in range(nz):
        for j, weight in enumerate((wro, wco)):
            local.append(
                pltpu.make_async_copy(
                    weight.at[pl.ds(k * lanes, lanes)],
                    wo.at[pl.ds((2 * k + j) * lanes, lanes), side_cols],
                    lsem.at[7 + 2 * k + j],
                )
            )
    local.append(
        pltpu.make_async_copy(
            table.at[pl.ds(aligned(y * rows, rows), rows)], tb, lsem.at[7 + 2 * nz]
        )
    )
    for copy in local:
        copy.start()

    barrier = pltpu.get_barrier_semaphore()
    for k in range(1, group):
        idx = (me + k) % group
        pl.semaphore_signal(
            barrier, inc=1, device_id=((idx // n_tp) * SIDES + y, idx % n_tp),
            device_id_type=pl.DeviceIdType.MESH,
        )
    pl.semaphore_signal(
        barrier, inc=1, device_id=other_y, device_id_type=pl.DeviceIdType.MESH
    )
    pl.semaphore_wait(barrier, group)

    def send_line(which, step, when):
        slot = xb.at[tp, which]
        cp.send(slot, slot, rx_line.at[which], dev(x, y, z + step, c), when)

    def share(which, when=None):
        slot = xb.at[tp, which]
        cp.send(slot, slot, rx_x.at[which], other_x, when)
        cp.send(slot, slot, rx_c.at[0, which], other_c, when)

    at_end = jnp.logical_or(z == 0, z == nz - 1)
    inside = jnp.logical_not(at_end)
    groups = ((0, (0, 1)), (1, (0, 1)), (2, (0,)), (2, (1,)))

    def send_weights(k, when=None):
        p, js = groups[k]
        for d in range(nz - 1, 0, -1):
            for zz, there in ((z - d, z >= d), (z + d, z + d < nz)):
                for j in js:
                    cp.send(
                        pairs[p][j].at[:, pl.ds(aligned(zz * lanes, lanes), lanes)],
                        wbuf.at[p, my_depth, pl.ds(j * lanes, lanes)],
                        rw.at[k, z], dev(x, y, zz, c), both(there, when),
                    )

    def await_weights(k):
        p, js = groups[k]
        at = pl.ds(js[0] * lanes, len(js) * lanes)
        for j in js:
            local[1 + 2 * p + j].wait()
        for d in range(1, nz):
            for zz, there in ((z - d, z >= d), (z + d, z + d < nz)):
                piece = wbuf.at[p, pl.ds(aligned(zz * depth, depth), depth), at]
                pl.when(there)(lambda piece=piece, zz=zz: arrive(piece, rw.at[k, zz]))

    cp.send(far_part, xb.at[tp, sp], rx_y, other_y)
    local[0].wait()
    send_line(sp, 1, z < nz - 1)
    send_line(sp, -1, z > 0)
    share(sp)
    for copy in local[7:-1]:
        copy.wait()
    beside = z * SIDES + 1 - y
    arrive(xb.at[tp, beside], rx_y)
    send_line(beside, 1, z < nz - 1)
    send_line(beside, -1, z > 0)
    share(beside)
    cp.send(wo.at[:, side_cols], wo.at[:, side_cols], r_wo, other_y)
    for d in range(1, nz):
        for side in (y, 1 - y):
            for zz, there, step, more in (
                (z - d, z >= d, 1, z < nz - 1), (z + d, z + d < nz, -1, z > 0),
            ):
                which = zz * SIDES + side
                slot = xb.at[tp, which]
                pl.when(there)(lambda slot=slot, which=which: arrive(slot, rx_line.at[which]))
                if d < nz - 1:
                    send_line(which, step, both(there, more))
                share(which, there)
        if d == 2:
            send_weights(0)
            send_weights(1, inside)
        if d == 3:
            send_weights(1, at_end)
            send_weights(2)
            send_weights(3)

    def pick(ref):
        here_lane = lax.broadcasted_iota(jnp.int32, ref.shape, 1) == z
        v = jnp.sum(jnp.where(here_lane, ref[...], 0.0), axis=1, keepdims=True)
        e = jnp.exp(-jnp.abs(v))
        small = e * (1.0 - e * (0.5 - e * (1.0 / 3.0 - e * 0.25)))
        return jnp.minimum(v, 0.0) - jnp.where(e < 1e-2, small, jnp.log(1.0 + e))

    log_f, log_b = pick(dec_f), pick(dec_b)
    index = lax.broadcasted_iota(jnp.int32, (blk, lanes), 0).astype(F32)
    dcol[0] = jnp.exp(log_f * (blk - 1.0 - index))
    dcol[1] = jnp.exp(log_b * index)
    dcol[2] = jnp.exp(log_f * (index + 1.0))
    dcol[3] = jnp.exp(log_b * (blk - index))
    across = lax.broadcasted_iota(jnp.int32, (blk, blk), 0) - lax.broadcasted_iota(
        jnp.int32, (blk, blk), 1
    )
    away = across.astype(F32)
    dmat[...] = jnp.exp(jnp.where(across >= 0, log_f * away, -log_b * away))
    leap_f, leap_b = jnp.exp(log_f * float(blk)), jnp.exp(log_b * float(blk))

    def gather_squares(q, first):
        at = pl.ds(aligned(q * part, part), part)
        gain_at = pl.ds(aligned(q * feats + y * part, part), part)

        def strip(i, carry):
            r = pl.ds(aligned(i * 16, 16), 16)
            v = xb[q, i // (blk // 16), pl.ds(aligned((i % (blk // 16)) * 16, 16), 16)]
            v = v.astype(F32)
            xg[r, at] = (v * gain[:, gain_at]).astype(BF16)
            w = v * v
            s = w[:, :lanes]
            for k in range(1, part // lanes):
                s = s + w[:, k * lanes : (k + 1) * lanes]
            ssq[r] = s if first else ssq[r] + s
            return carry

        lax.fori_loop(0, SIDES * rows // 16, strip, 0)

    far_q = other_x[1]
    for d in range(nz):
        for side in (y, 1 - y):
            for zz, there in ((z - d, z >= d),) if d == 0 else ((z - d, z >= d), (z + d, z + d < nz)):
                which = zz * SIDES + side
                slot = xb.at[far_q, which]
                pl.when(there)(lambda slot=slot, which=which: arrive(slot, rx_x.at[which]))
                cp.send(slot, slot, rx_c.at[1, which], other_c, there)
    gather_squares(tp, True)
    gather_squares(far_q, False)
    for k, q in enumerate((other_c[1], dev(1 - x, y, z, 1 - c)[1])):
        for which in range(n_sp):
            arrive(xb.at[q, which], rx_c.at[k, which])
        gather_squares(q, False)

    width = n_tp * feats

    def lay(i, carry):
        block = ssq[pl.ds(aligned(i * 128, 128), 128)].T
        sqs[pl.ds(i, 1)] = jnp.sum(block, axis=0, keepdims=True)
        return carry

    lax.fori_loop(0, SIDES * count, lay, 0)
    cp.send(sqs, sqr, r_sq, other_y)

    def project(k):
        p, js = groups[k]
        wide = len(js) * lanes
        at = pl.ds(js[0] * lanes, wide)
        tall = rows // 2
        for h in range(2):
            r = pl.ds(aligned((1 - y) * rows + h * tall, tall), tall)
            acc = jnp.dot(xg[r], wbuf[p, :, at], preferred_element_type=F32)
            to = pl.ds(h * tall, tall)
            pso[p, to, at] = acc.astype(BF16)
            cp.send(pso.at[p, to, at], pre.at[p, to, at], r_p.at[k, h], other_y)

        def body(h, carry):
            r = pl.ds(aligned(y * rows + h * tall, tall), tall)
            own[p, pl.ds(aligned(h * tall, tall), tall), at] = jnp.dot(
                xg[r], wbuf[p, :, at], preferred_element_type=F32
            )
            return carry

        lax.fori_loop(0, 2, body, 0)

    def combine(k):
        p, js = groups[k]
        at = pl.ds(js[0] * lanes, len(js) * lanes)
        tall = rows // 2
        for h in range(2):
            arrive(pre.at[p, pl.ds(h * tall, tall), at], r_p.at[k, h])

        def body(i, carry):
            r = pl.ds(aligned(i * 128, 128), 128)
            for j in js:
                lane = pl.ds(j * lanes, lanes)
                total = (own[p, r, lane] + pre[p, r, lane].astype(F32)) * scl[r]
                pj[p, r, lane] = total.astype(BF16)
            return carry

        lax.fori_loop(0, count, body, 0)

    pad = 16
    edge_at = pl.ds(aligned((1 - y) * (rows - pad), pad), pad)
    edge_from = pl.ds(aligned(y * (rows - pad), pad), pad)

    def row_scales():
        arrive(sqr, r_sq)
        sqt[...] = lax.rsqrt((sqs[...] + sqr[...]) / width + EPS)

        def body(i, carry):
            row = jnp.broadcast_to(sqt[pl.ds(y * count + i, 1)], (128, lanes))
            scl[pl.ds(aligned(i * 128, 128), 128)] = row.T
            return carry

        lax.fori_loop(0, count, body, 0)
        turned_edge[...] = jnp.broadcast_to(sqt[pl.ds(count - y, 1)], (128, lanes)).T

    def unit_of(a, b):
        a, b = a.astype(BF16).astype(F32), b.astype(BF16).astype(F32)
        return (a * jax.nn.sigmoid(b)).astype(BF16).astype(F32)

    def edge_unit():
        arrive(er, r_e)
        total = pso[0, edge_from].astype(F32) + er[...].astype(F32)
        scale = turned_edge[pl.ds(aligned(y * (128 - pad), pad), pad)]
        unit = unit_of(total[:, :lanes] * scale, total[:, lanes:] * scale)
        ubuf[pl.ds(0, pad)] = jnp.where(y == 1, unit, 0.0)
        ubuf[pl.ds(pad + rows, pad)] = jnp.where(y == 0, unit, 0.0)

    def gate(i, carry):
        r = aligned(i * 128, 128)
        a = pj[0, pl.ds(r, 128), pl.ds(0, lanes)].astype(F32)
        b = pj[0, pl.ds(r, 128), pl.ds(lanes, lanes)].astype(F32)
        ubuf[pl.ds(aligned(r + pad, 16), 128)] = (a * jax.nn.sigmoid(b)).astype(BF16).astype(F32)
        return carry

    wts = taps[:, my_cols]
    bias = dbias[:, my_cols]
    reach = (KERNEL - 1) // 2

    def convolve(block, carry):
        for half in range(2):
            r = aligned(block * 128 + half * 64, 64)
            acc = jnp.broadcast_to(bias, (64, lanes))
            for t in range(KERNEL):
                acc = acc + wts[t : t + 1] * ubuf[pl.ds(r + (pad - reach + t), 64)]
            fbuf[pl.ds(r, 64)] = acc
        turned = fbuf[pl.ds(aligned(block * 128, 128), 128)].T
        st[pl.ds(block, 1)] = jnp.sum(turned, axis=0, keepdims=True)
        st[pl.ds(count + block, 1)] = jnp.sum(turned * turned, axis=0, keepdims=True)
        return carry

    await_weights(0)
    project(0)
    es[...] = own[0, edge_at].astype(BF16)
    cp.send(es, er, r_e, other_y)
    row_scales()
    combine(0)
    edge_unit()
    lax.fori_loop(0, count, gate, 0)
    lax.fori_loop(0, count, convolve, 0)
    for k in range(1, group):
        idx = (me + k) % group
        cp.send(
            st, sr.at[me], r_stat.at[me], ((idx // n_tp) * SIDES + y, idx % n_tp)
        )
    sr[me] = st[...]

    await_weights(1)
    project(1)
    for k in range(1, group):
        idx = (me + k) % group
        arrive(sr.at[idx], r_stat.at[idx])
    sums = sr[0]
    for k in range(1, group):
        sums = sums + sr[k]
    st_mean = sums[:count] / CONV_WIDTH
    st_scale = lax.rsqrt(sums[count:] / CONV_WIDTH - st_mean * st_mean + EPS)
    conv_cols = pl.ds(aligned(z * 2 * lanes + lanes, lanes), lanes)
    ret_cols = pl.ds(aligned(z * 2 * lanes, lanes), lanes)
    gain_c, bias_c = cg[:, my_cols], cb[:, my_cols]
    for i in range(count):
        r = pl.ds(i * 128, 128)
        mean = jnp.broadcast_to(st_mean[i : i + 1], (128, lanes)).T
        scale = jnp.broadcast_to(st_scale[i : i + 1], (128, lanes)).T
        level = (fbuf[r] - mean) * scale * gain_c + bias_c
        mix[r, conv_cols] = (level * jax.nn.sigmoid(level)).astype(BF16)

    def mix_part(zz, r, conv):
        start = zz * 2 * lanes + (lanes if conv else 0)
        return mix.at[r, pl.ds(aligned(start, lanes), lanes)]

    def mix_send(zz, r, conv, sem, step, when):
        cp.send(mix_part(zz, r, conv), mix_part(zz, r, conv), sem, dev(x, y, z + step, c), when)

    def mix_hop(d, r, conv, sems):
        low, high = z - d, z + d
        has_low, has_high = low >= 0, high < nz
        pl.when(has_low)(lambda: arrive(mix_part(low, r, conv), sems.at[low]))
        if d < nz - 1:
            mix_send(low, r, conv, sems.at[low], 1, both(has_low, z < nz - 1))
        pl.when(has_high)(lambda: arrive(mix_part(high, r, conv), sems.at[high]))
        if d < nz - 1:
            mix_send(high, r, conv, sems.at[high], -1, both(has_high, z > 0))

    every = pl.ds(0, rows)
    mix_send(z, every, True, rm_c.at[z], 1, z < nz - 1)
    mix_send(z, every, True, rm_c.at[z], -1, z > 0)

    first_half = lax.broadcasted_iota(jnp.int32, (blk, lanes), 1) < lanes // 2

    def turn(v, r):
        t = tb[r]
        rolled = pltpu.roll(t, lanes // 2, 1)
        cosine = jnp.where(first_half, t, rolled)
        sine = jnp.where(first_half, -rolled, t)
        return (v * cosine + pltpu.roll(v, lanes // 2, 1) * sine).astype(BF16)

    def states(i, carry):
        r = pl.ds(aligned(i * blk, blk), blk)
        keys = turn(pj[1, r, pl.ds(0, lanes)].astype(F32), r)
        kr[r] = keys
        wide = keys.astype(F32)
        both_ways = jnp.concatenate(
            [(wide * dcol[0]).astype(BF16), (wide * dcol[1]).astype(BF16)], axis=1
        )
        state = lax.dot_general(
            both_ways, pj[1, r, pl.ds(lanes, lanes)], (((0,), (0,)), ((), ())),
            preferred_element_type=F32,
        )
        ef[i] = state[:lanes]
        eb[i] = state[lanes:]
        return carry

    await_weights(2)
    project(2)
    combine(1)
    local[-1].wait()
    lax.fori_loop(0, chunks, states, 0)
    run = ef[0]
    ef[0] = jnp.zeros_like(run)
    for i in range(1, chunks):
        mine = ef[i]
        ef[i] = run
        run = run * leap_f + mine
    back = eb[chunks - 1]
    eb[chunks - 1] = jnp.zeros_like(back)
    for i in range(chunks - 2, -1, -1):
        mine = eb[i]
        eb[i] = back
        back = back * leap_b + mine
    ts[...] = jnp.where(y == 0, run, back).astype(BF16)
    cp.send(ts, tr, r_state, other_y)
    await_weights(3)
    project(3)
    arrive(tr, r_state)
    entering = tr[...].astype(F32)
    entering_f = jnp.where(y == 1, entering, 0.0)
    entering_b = jnp.where(y == 0, entering, 0.0)
    for i in range(chunks):
        ef[i] = ef[i] + entering_f
        entering_f = entering_f * leap_f
    for i in range(chunks - 1, -1, -1):
        eb[i] = eb[i] + entering_b
        entering_b = entering_b * leap_b
    combine(2)
    mix_hop(1, every, True, rm_c)
    gain_r, bias_r = gg[:, my_cols], gb[:, my_cols]

    def retain(i, carry):
        r = pl.ds(aligned(i * blk, blk), blk)
        queries = turn(pj[2, r, pl.ds(0, lanes)].astype(F32), r)
        keys, values = kr[r], pj[1, r, pl.ds(lanes, lanes)]
        scores = lax.dot_general(
            queries, keys, (((1,), (1,)), ((), ())), preferred_element_type=F32
        )
        scores = (scores * dmat[...]).astype(BF16)
        inner = jnp.dot(scores, values, preferred_element_type=F32)
        enter = jnp.concatenate([ef[i], eb[i]], axis=1).astype(BF16)
        carried = jnp.dot(queries, enter, preferred_element_type=F32)
        retained = inner + carried[:, :lanes] * dcol[2] + carried[:, lanes:] * dcol[3]
        mean = jnp.mean(retained, axis=-1, keepdims=True)
        centered = retained - mean
        spread = jnp.mean(centered * centered, axis=-1, keepdims=True)
        fbuf[r] = centered * lax.rsqrt(spread + EPS) * gain_r + bias_r
        return carry

    lax.fori_loop(0, chunks, retain, 0)
    combine(3)

    spans = [
        pl.ds(aligned((i + (1 - y) * (1 - 2 * (i % SIDES))) * blk, blk), blk)
        for i in range(chunks)
    ]

    def ret_gate(i):
        g = pj[2, spans[i], pl.ds(lanes, lanes)].astype(F32)
        mix[spans[i], ret_cols] = (g * jax.nn.sigmoid(g) * fbuf[spans[i]]).astype(BF16)

    def ret_send(i):
        mix_send(z, spans[i], False, rm_r.at[i, z], 1, z < nz - 1)
        mix_send(z, spans[i], False, rm_r.at[i, z], -1, z > 0)

    def ret_hop(d, i):
        mix_hop(d, spans[i], False, rm_r.at[i])

    for i in range(chunks):
        ret_gate(i)
        if i < 2:
            ret_send(i)
    mix_hop(2, every, True, rm_c)

    def multiply(i):
        acc = jnp.dot(mix[spans[i]], wo[...], preferred_element_type=F32)
        for t in range(n_tp):
            ps[i, t % CORES, t // CORES] = acc[t * fine : (t + 1) * fine].astype(BF16)
        cp.send(ps.at[i, 1 - c], r1.at[i], rs1.at[i], other_c)

    def add_cores(i):
        arrive(r1.at[i], rs1.at[i])
        s2[i] = (ps[i, c, 1 - x].astype(F32) + r1[i, 1 - x].astype(F32)).astype(BF16)
        cp.send(s2.at[i], r2.at[i], rs2.at[i], other_x)

    def deliver(buf, i, z_to):
        apart = z_to != z
        cp.send(buf.at[i], ob.at[z], ro.at[z], dev(x, y, z_to, c), apart)

        @pl.when(jnp.logical_not(apart))
        def _():
            ob[z] = buf[i]

    def add_far(i):
        arrive(r2.at[i], rs2.at[i])
        total = ps[i, c, x].astype(F32) + r1[i, x].astype(F32) + r2[i].astype(F32)
        os_[i] = total.astype(BF16)
        if i % SIDES == 0:
            cp.send(os_.at[i], oy.at[i // SIDES], roy.at[i // SIDES], other_y)
        else:
            deliver(os_, i, SIDES * y + i // SIDES)

    def relay(k):
        arrive(oy.at[k], roy.at[k])
        deliver(oy, k, SIDES * (1 - y) + k)

    ret_hop(1, 0)
    ret_send(2)
    ret_hop(1, 1)
    ret_hop(2, 0)
    ret_send(3)
    ret_hop(1, 2)
    ret_hop(2, 1)
    mix_hop(3, every, True, rm_c)
    arrive(wo.at[:, far_cols], r_wo)
    ret_hop(3, 0)
    multiply(0)
    ret_hop(1, 3)
    ret_hop(2, 2)
    ret_hop(3, 1)
    multiply(1)
    add_cores(0)
    ret_hop(2, 3)
    ret_hop(3, 2)
    multiply(2)
    add_cores(1)
    add_far(0)
    ret_hop(3, 3)
    multiply(3)
    add_cores(2)
    add_far(1)
    relay(0)
    add_cores(3)
    add_far(2)
    add_far(3)
    relay(1)
    for zz in range(nz):
        @pl.when(zz != z)
        def _():
            arrive(ob.at[zz], ro.at[zz])

        out[:, pl.ds(zz * cols, cols)] = ob[zz]
    cp.drain()


def fused(
    hidden_states, norm_gain, query_weight, key_weight, value_weight, output_gate_weight,
    unit_input_weight, unit_gate_weight, decay_forward, decay_backward, group_gain, group_bias,
    depth_kernel, depth_bias, channel_gain, channel_bias, retention_out_weight,
    convolution_out_weight,
):
    n_sp, n_tp = lax.axis_size("sp"), lax.axis_size("tp")
    nz = n_sp // SIDES
    blk, feats = hidden_states.shape
    part = feats // SIDES
    depth = query_weight.shape[0]
    rows = nz * blk
    lanes = HEAD_DIM
    cols = SIDES * retention_out_weight.shape[1]
    fine = blk // n_tp
    half_dim = lanes // 2
    inverse = np.float32(THETA) ** (-np.arange(half_dim, dtype=np.float32) / np.float32(half_dim))
    angles = np.arange(SIDES * rows, dtype=np.float32)[:, None] * inverse.astype(np.float32)[None]
    table = np.concatenate([np.cos(angles.astype(np.float64)), np.sin(angles.astype(np.float64))], 1)
    table = jnp.asarray(table.astype(np.float32))
    count = rows // 128

    def row(v):
        return v.reshape(1, v.shape[0])

    any_, vmem = pl.BlockSpec(memory_space=pl.ANY), pl.BlockSpec(memory_space=pltpu.VMEM)
    dma = pltpu.SemaphoreType.DMA
    group = nz * n_tp
    return pl.pallas_call(
        functools.partial(fused_kernel, nz, n_tp),
        out_shape=jax.ShapeDtypeStruct((fine, nz * cols), BF16),
        in_specs=[any_, vmem] + [any_] * 6 + [vmem] * 8 + [any_] * 3,
        out_specs=vmem,
        scratch_shapes=[
            pltpu.VMEM((n_tp, n_sp, blk, part), BF16),
            pltpu.VMEM((SIDES * rows, n_tp * part), BF16),
            pltpu.VMEM((SIDES * rows, lanes), F32),
            pltpu.VMEM((SIDES * count, lanes), F32),
            pltpu.VMEM((SIDES * count, lanes), F32),
            pltpu.VMEM((SIDES * count, lanes), F32),
            pltpu.VMEM((rows, lanes), F32),
            pltpu.VMEM((128, lanes), F32),
            pltpu.VMEM((3, nz * depth, 2 * lanes), BF16),
            pltpu.VMEM((3, rows, 2 * lanes), F32),
            pltpu.VMEM((3, rows, 2 * lanes), BF16),
            pltpu.VMEM((3, rows, 2 * lanes), BF16),
            pltpu.VMEM((3, rows, 2 * lanes), BF16),
            pltpu.VMEM((16, 2 * lanes), BF16),
            pltpu.VMEM((16, 2 * lanes), BF16),
            pltpu.VMEM((rows + 32, lanes), F32),
            pltpu.VMEM((rows, lanes), F32),
            pltpu.VMEM((2 * count, lanes), F32),
            pltpu.VMEM((group, 2 * count, lanes), F32),
            pltpu.VMEM((rows, lanes), F32),
            pltpu.VMEM((nz, lanes, lanes), F32),
            pltpu.VMEM((nz, lanes, lanes), F32),
            pltpu.VMEM((lanes, lanes), BF16),
            pltpu.VMEM((lanes, lanes), BF16),
            pltpu.VMEM((rows, lanes), BF16),
            pltpu.VMEM((4, blk, lanes), F32),
            pltpu.VMEM((blk, blk), F32),
            pltpu.VMEM((rows, nz * 2 * lanes), BF16),
            pltpu.VMEM((nz * 2 * lanes, cols), BF16),
            pltpu.VMEM((nz, CORES, n_tp // CORES, fine, cols), BF16),
            pltpu.VMEM((nz, n_tp // CORES, fine, cols), BF16),
            pltpu.VMEM((nz, fine, cols), BF16),
            pltpu.VMEM((nz, fine, cols), BF16),
            pltpu.VMEM((nz, fine, cols), BF16),
            pltpu.VMEM((nz, fine, cols), BF16),
            pltpu.VMEM((SIDES, fine, cols), BF16),
            dma((300,)),
            dma((8 + 2 * nz,)),
            dma, dma((n_sp,)), dma((n_sp,)), dma((2, n_sp)),
            dma((4, nz)), dma, dma, dma((4, 2)), dma, dma((group,)), dma,
            dma((nz,)), dma((nz, nz)),
            dma((nz,)), dma((nz,)), dma((nz,)), dma((SIDES,)),
        ],
        compiler_params=pltpu.CompilerParams(
            collective_id=0, has_side_effects=True, vmem_limit_bytes=60 * 1024 * 1024
        ),
    )(
        hidden_states, row(norm_gain), query_weight, key_weight, value_weight, output_gate_weight,
        unit_input_weight, unit_gate_weight, row(decay_forward), row(decay_backward),
        row(group_gain), row(group_bias), depth_kernel, row(depth_bias), row(channel_gain),
        row(channel_bias), retention_out_weight, convolution_out_weight, table,
    )


def with_halo(cells, sides, width):
    for axis, dim in sides:
        count = lax.axis_size(axis)
        ends = count - 1
        head = lax.slice_in_dim(cells, 0, width, axis=dim)
        tail = lax.slice_in_dim(cells, cells.shape[dim] - width, cells.shape[dim], axis=dim)
        cells = jnp.concatenate(
            [
                lax.ppermute(tail, axis, [(i, (i + 1) % count) for i in range(ends)]),
                cells,
                lax.ppermute(head, axis, [((i + 1) % count, i) for i in range(ends)]),
            ],
            axis=dim,
        )
    return cells


def rotate_at(rows, positions):
    half_dim = rows.shape[-1] // 2
    inverse = THETA ** (-jnp.arange(half_dim, dtype=jnp.float32) / half_dim)
    angles = positions.astype(jnp.float32)[:, None] * inverse[None, :]
    cosine = jnp.cos(angles)[:, None, :]
    sine = jnp.sin(angles)[:, None, :]
    widened = rows.astype(jnp.float32)
    first_half = widened[..., :half_dim]
    second_half = widened[..., half_dim:]
    turned = jnp.concatenate(
        [first_half * cosine - second_half * sine, second_half * cosine + first_half * sine],
        axis=-1,
    )
    return turned.astype(jnp.bfloat16)


def to_blocks(rows):
    return rows.reshape(rows.shape[0] // BLOCK, BLOCK, rows.shape[1], rows.shape[2]).transpose(
        2, 0, 1, 3
    )


def from_blocks(blocks):
    return blocks.transpose(1, 2, 0, 3).reshape(
        blocks.shape[1] * blocks.shape[2], blocks.shape[0], blocks.shape[3]
    )


def blockwise(queries, key_rows, values, log_decay, include_diag):
    block_len = queries.shape[2]
    position = jnp.arange(block_len, dtype=jnp.float32)
    distance = position[:, None] - position[None, :]
    allowed = distance >= 0 if include_diag else distance > 0
    inside = jnp.where(
        allowed[None], jnp.exp(log_decay[:, None, None] * jnp.maximum(distance, 0.0)[None]), 0.0
    )
    query_wide = queries.astype(jnp.float32)
    key_wide = key_rows.astype(jnp.float32)
    value_wide = values.astype(jnp.float32)
    scores = (
        jnp.einsum("hnqd,hnkd->hnqk", query_wide, key_wide, precision=lax.Precision.HIGHEST)
        * inside[:, None]
    )
    inner_part = jnp.einsum("hnqk,hnkd->hnqd", scores, value_wide, precision=lax.Precision.HIGHEST)
    toward_end = jnp.exp(log_decay[:, None] * (block_len - 1.0 - position)[None])
    block_states = jnp.einsum(
        "hnkd,hnke->hnde",
        key_wide * toward_end[:, None, :, None],
        value_wide,
        precision=lax.Precision.HIGHEST,
    )
    block_decay = jnp.exp(log_decay * block_len)[:, None, None]

    def advance(state_now, block_state):
        return (block_decay * state_now + block_state, state_now)

    initial = jnp.zeros(
        (block_states.shape[0], block_states.shape[2], block_states.shape[3]), jnp.float32
    )
    final_state, earlier = lax.scan(advance, initial, jnp.moveaxis(block_states, 1, 0))
    earlier = jnp.moveaxis(earlier, 0, 1)
    from_start = jnp.exp(log_decay[:, None] * (position + 1.0)[None])
    cross_part = jnp.einsum(
        "hnqd,hnde->hnqe",
        query_wide * from_start[:, None, :, None],
        earlier,
        precision=lax.Precision.HIGHEST,
    )
    return (inner_part + cross_part, final_state)


def group_norm(retained, group_gain, group_bias, gate_rows):
    row_mean = jnp.mean(retained, axis=-1, keepdims=True)
    centered = retained - row_mean
    variance = jnp.mean(centered * centered, axis=-1, keepdims=True)
    scaled = (centered * lax.rsqrt(variance + EPS)).reshape(retained.shape[0], -1)
    scaled = scaled * group_gain[None, :] + group_bias[None, :]
    return (jax.nn.silu(gate_rows.astype(jnp.float32)) * scaled).astype(jnp.bfloat16)


def shards_general(
    hidden_states,
    norm_gain,
    query_weight,
    key_weight,
    value_weight,
    output_gate_weight,
    unit_input_weight,
    unit_gate_weight,
    decay_forward,
    decay_backward,
    group_gain,
    group_bias,
    depth_kernel,
    depth_bias,
    channel_gain,
    channel_bias,
    retention_out_weight,
    convolution_out_weight,
):
    row_total = hidden_states.shape[0]
    whole = lax.all_gather(hidden_states, "tp", axis=1, tiled=True)
    widened = whole.astype(jnp.float32)
    normed = (
        widened
        * lax.rsqrt(jnp.mean(widened * widened, axis=-1, keepdims=True) + EPS)
        * norm_gain[None, :]
    ).astype(jnp.bfloat16)
    slabs = (
        lax.all_gather(query_weight, "sp", axis=0, tiled=True),
        lax.all_gather(key_weight, "sp", axis=0, tiled=True),
        lax.all_gather(value_weight, "sp", axis=0, tiled=True),
        lax.all_gather(output_gate_weight, "sp", axis=0, tiled=True),
        lax.all_gather(unit_input_weight, "sp", axis=0, tiled=True),
        lax.all_gather(unit_gate_weight, "sp", axis=0, tiled=True),
    )
    summed = tuple((jnp.dot(normed, slab, preferred_element_type=jnp.float32) for slab in slabs))
    proj_q, proj_k, proj_v, proj_g, proj_a, proj_b = tuple(
        (part_sum.astype(jnp.bfloat16) for part_sum in summed)
    )
    head_count = proj_q.shape[1] // HEAD_DIM
    device = lax.axis_index("sp")
    positions = device * row_total + jnp.arange(row_total, dtype=jnp.int32)
    queries = rotate_at(proj_q.reshape(row_total, head_count, HEAD_DIM), positions)
    key_rows = rotate_at(proj_k.reshape(row_total, head_count, HEAD_DIM), positions)
    values = proj_v.reshape(row_total, head_count, HEAD_DIM)
    log_forward = jax.nn.log_sigmoid(decay_forward)
    log_backward = jax.nn.log_sigmoid(decay_backward)
    ahead_local, state_ahead = blockwise(
        to_blocks(queries), to_blocks(key_rows), to_blocks(values), log_forward, True
    )
    behind_local, state_behind = blockwise(
        to_blocks(queries[::-1]),
        to_blocks(key_rows[::-1]),
        to_blocks(values[::-1]),
        log_backward,
        False,
    )
    slabs = (
        lax.all_gather(state_ahead[None].astype(jnp.bfloat16), "sp", axis=0, tiled=True).astype(
            jnp.float32
        ),
        lax.all_gather(state_behind[None].astype(jnp.bfloat16), "sp", axis=0, tiled=True).astype(
            jnp.float32
        ),
    )
    source = jnp.arange(slabs[0].shape[0], dtype=jnp.int32)
    gap_ahead = device - 1 - source
    gap_behind = source - device - 1
    weight_ahead = jnp.where(
        gap_ahead[:, None] >= 0,
        jnp.exp(
            log_forward[None, :]
            * row_total
            * jnp.maximum(gap_ahead, 0).astype(jnp.float32)[:, None]
        ),
        0.0,
    )
    weight_behind = jnp.where(
        gap_behind[:, None] >= 0,
        jnp.exp(
            log_backward[None, :]
            * row_total
            * jnp.maximum(gap_behind, 0).astype(jnp.float32)[:, None]
        ),
        0.0,
    )
    enter_ahead = jnp.zeros_like(state_ahead) + jnp.einsum(
        "jh,jhde->hde", weight_ahead, slabs[0], precision=lax.Precision.HIGHEST
    )
    enter_behind = jnp.zeros_like(state_behind) + jnp.einsum(
        "jh,jhde->hde", weight_behind, slabs[1], precision=lax.Precision.HIGHEST
    )
    local_position = jnp.arange(row_total, dtype=jnp.float32)
    lift_ahead = jnp.exp(log_forward[None, :] * (local_position + 1.0)[:, None])
    lift_behind = jnp.exp(log_backward[None, :] * (row_total - local_position)[:, None])
    query_wide = queries.astype(jnp.float32)
    carried = jnp.einsum(
        "shd,hde->she",
        query_wide * lift_ahead[:, :, None],
        enter_ahead,
        precision=lax.Precision.HIGHEST,
    )
    carried = carried + jnp.einsum(
        "shd,hde->she",
        query_wide * lift_behind[:, :, None],
        enter_behind,
        precision=lax.Precision.HIGHEST,
    )
    retained = from_blocks(ahead_local) + from_blocks(behind_local)[::-1] + carried
    retention_rows = group_norm(retained, group_gain, group_bias, proj_g)
    unit = (proj_a.astype(jnp.float32) * jax.nn.sigmoid(proj_b.astype(jnp.float32))).astype(
        jnp.bfloat16
    )
    half_kernel = (KERNEL - 1) // 2
    padded = with_halo(unit, (("sp", 0),), half_kernel)
    filtered = jnp.broadcast_to(depth_bias[None, :], (row_total, unit.shape[1]))
    for offset in range(KERNEL):
        filtered = filtered + depth_kernel[offset][None, :] * padded[
            offset : offset + row_total
        ].astype(jnp.float32)
    row_sum, row_squares = lax.psum(
        (jnp.sum(filtered, axis=1), jnp.sum(filtered * filtered, axis=1)), "tp"
    )
    row_mean = (row_sum / CONV_WIDTH)[:, None]
    variance = (row_squares / CONV_WIDTH)[:, None] - row_mean * row_mean
    leveled = (filtered - row_mean) * lax.rsqrt(variance + EPS) * channel_gain[
        None, :
    ] + channel_bias[None, :]
    convolution_rows = jax.nn.silu(leveled).astype(jnp.bfloat16)
    retention_full, convolution_full = (
        lax.all_gather(retention_out_weight, "sp", axis=1, tiled=True),
        lax.all_gather(convolution_out_weight, "sp", axis=1, tiled=True),
    )
    return lax.psum_scatter(
        (
            jnp.dot(retention_rows, retention_full, preferred_element_type=jnp.float32)
            + jnp.dot(convolution_rows, convolution_full, preferred_element_type=jnp.float32)
        ).astype(jnp.bfloat16),
        "tp",
        scatter_dimension=0,
        tiled=True,
    )


def solution(mesh):
    n_sp, n_tp = mesh.shape["sp"], mesh.shape["tp"]
    fits = n_tp == 2 * CORES and n_sp % SIDES == 0
    fits = fits and n_sp // SIDES * n_tp * HEAD_DIM == CONV_WIDTH and n_sp // SIDES == n_tp
    placed = (
        P("sp", "tp"),
        P(),
        P("sp", "tp"),
        P("sp", "tp"),
        P("sp", "tp"),
        P("sp", "tp"),
        P("sp", "tp"),
        P("sp", "tp"),
        P("tp"),
        P("tp"),
        P("tp"),
        P("tp"),
        P(None, "tp"),
        P("tp"),
        P("tp"),
        P("tp"),
        P("tp", "sp"),
        P("tp", "sp"),
    )
    return jax.shard_map(
        fused if fits else shards_general,
        mesh=mesh, in_specs=placed, out_specs=P(("sp", "tp"), None), check_vma=False
    )
```
